32 devices in a mesh: sp: 8 (over z, core), tp: 4 (over y, x).
Axes of the slice: x: 2, y: 2, z: 4, core: 2. Of those that a mesh axis runs over, the one named last changes fastest.
Arguments:
- stream: bfloat16 [2048, 1024], P('tp', 'sp')
- values_in: bfloat16 [1024, 1024], P('tp', 'sp'), may hold values from -6 to 6
- in_gate: bfloat16 [1024, 1024], P('tp', 'sp'), may hold values from -6 to 6
- out_gate: bfloat16 [1024, 1024], P('tp', 'sp'), may hold values from -6 to 6
- documents: int32 [1024], P('sp'), may hold values from 0 to 15, never falling along the last dimension, each value on 1 to 256 neighbouring positions
- conv_taps: float32 [3, 1024], P(None, 'tp'), may hold values from -3.5 to 3.5
- head_gain: float32 [1024], P('tp'), may hold values from 0.1 to 1.9
- mix_weight: bfloat16 [1024, 2048], P('tp'), may hold values from -0.25 to 0.25
- norm_gain: float32 [2048], P('tp'), may hold values from 0.1 to 1.9
- routes: int32 [1024, 4], P('sp'), may hold values from 0 to 7, all different within a row; in each aligned block of 128 rows (0 to 127, 128 to 255, ...) at most 96 rows name the same one
- route_weight: float32 [1024, 4], P('sp'), may hold values from 0.2 to 1
- expert_gate: bfloat16 [8, 2048, 2048], P('sp', None, 'tp'), may hold values from -0.125 to 0.125
- expert_up: bfloat16 [8, 2048, 2048], P('sp', None, 'tp'), may hold values from -0.125 to 0.125
- expert_down: bfloat16 [8, 2048, 2048], P('sp', None, 'tp'), may hold values from -0.125 to 0.125
- shared_gate: bfloat16 [2048, 2048], P(None, 'tp'), may hold values from -0.125 to 0.125
- shared_up: bfloat16 [2048, 2048], P(None, 'tp'), may hold values from -0.125 to 0.125
- shared_down: bfloat16 [2048, 2048], P('tp'), may hold values from -0.1875 to 0.1875
Outputs:
- layer_out: bfloat16 [2048, 1024], P('tp', 'sp')
The draws below stay inside these ranges and needn't reach their ends.
Inputs may be any that keep to these rules, and one draw needn't show every extreme that they name: `routes`: each row names 4 different experts. In each aligned block of 128 rows no expert is named by more than 96 rows, a bound that some block reaches. `documents`: document numbers never fall along the positions; each document has 1 to 256 positions, and one has exactly that many.
All inputs are finite; a program needn't handle non-finite values.
Results may differ from the reference program's by a relative error of at most 0.015.
Values may be sent and summed in bfloat16 or wider, within the bound.
A program may use at most 64 MiB of HBM per device.

```python
import math
import jax
import jax.numpy as jnp
import numpy as np
from jax import lax

D = 2048
HEADS = 16
HEAD = 64
CW = 1024
FE = 2048
FS = 2048
TOP_K = 4
TOK_DEV = 128
TOKENS = 1024
EXPERTS = 8
CAP = 96
N_SP = 8
N_TP = 4


def draw_stream(key, part):
    first = jax.random.fold_in(jax.random.fold_in(key, 11), 0)
    feature_scale = 0.5 * 4.0 ** (jnp.arange(D, dtype=jnp.float32) / D)
    base = jax.random.normal(first, (D, TOKENS), jnp.float32)
    return (base * feature_scale[:, None]).astype(jnp.bfloat16)


def with_spikes(entries, key, source, target, blocks, factor):
    owner, partner = [(jnp.arange(entries.shape[position]) // (entries.shape[position] // blocks)).reshape([-1 if axis == position else 1 for axis in range(entries.ndim)]) for position in (source, target)]
    chosen = jax.random.permutation(key, blocks)[partner]
    strong = (owner == chosen) | (owner == (partner + blocks // 2) % blocks)
    return jnp.where(strong, factor * entries, entries)


def steps_of(own_key, shape, pieces, low, high):
    factor_of = 1.0
    for dim, blocks in pieces:
        heights = jax.random.uniform(jax.random.fold_in(jax.random.fold_in(own_key, 6), dim), (blocks,), jnp.float32, low / len(pieces), high / len(pieces))
        factor_of = factor_of * jnp.repeat(jnp.exp(heights), shape[dim] // blocks).reshape((-1,) + (1,) * (len(shape) - 1 - dim))
    return factor_of


def profile(number_of, total, reach, slope):
    weights = [(1 << 20) // math.isqrt(rank ** slope) + 1 for rank in range(2, number_of + 1)]
    spare, counts = total - reach - (number_of - 1), [1] * (number_of - 1)
    while spare > 0:
        free = [i for i in range(number_of - 1) if counts[i] < reach]
        pool, budget = sum([weights[i] for i in free]), spare
        for i in free:
            addition = min(reach - counts[i], max(1, budget * weights[i] // pool), spare)
            counts[i] = counts[i] + addition
            spare = spare - addition
    return np.array([reach] + counts)


def uneven_parts(own_key, number_of, total, most, lean):
    if number_of == 2:
        one = jax.random.randint(own_key, (), max(1, total - most), min(most, total - 1) + 1)
        return jnp.stack([one, total - one])
    lengths = jnp.asarray(profile(number_of, total, most, lean), jnp.int32)
    twos = (number_of - 1) // 2
    donor, receiver = lengths[1:1 + 2 * twos:2], lengths[2:2 + 2 * twos:2]
    room = jnp.minimum(donor - 1, most - receiver)
    passed = jax.random.randint(jax.random.fold_in(own_key, 1), (twos,), 0, 1 << 20) % (room + 1)
    lengths = lengths.at[1:1 + 2 * twos:2].set(donor - passed).at[2:2 + 2 * twos:2].set(receiver + passed)
    return lengths[jax.random.permutation(jax.random.fold_in(own_key, 2), number_of)]


def deal_out(stream_key, own, number, rows, amount, top, reach, lean):
    ranking = jax.random.permutation(stream_key, amount)
    heavy_load, usual = portions_of(amount, rows * top, reach, lean, True), portions_of(amount, rows * top, reach, lean, False)
    places = jnp.arange(amount)

    def named(lengths, turn):
        used = int((lengths > 0).sum())
        fixed = max(1, used // 4)
        passed = fixed + (places - fixed + turn * (used - fixed)) % max(1, amount - fixed)
        return jnp.zeros((amount,), jnp.int32).at[ranking[jnp.where(places < fixed, places, passed)]].set(jnp.asarray(lengths, jnp.int32))

    lengths = jnp.where(number % 4 == 0, named(heavy_load, number // 4), named(usual, number - number // 4 - 1))
    mixed = jax.random.permutation(jax.random.fold_in(own, 3), amount)
    source_of, taker = mixed[0:amount // 2 * 2:2], mixed[1:amount // 2 * 2:2]
    room = jnp.minimum(lengths[source_of] - 1, reach - lengths[taker]) // 2
    room = jnp.where((source_of == ranking[0]) | (taker == ranking[0]) | (lengths[taker] == 0), 0, jnp.maximum(room, 0))
    passed = jax.random.randint(jax.random.fold_in(own, 4), (amount // 2,), 0, 1 << 20) % (room + 1)
    lengths = lengths.at[source_of].add(-passed).at[taker].add(passed)
    items = jnp.searchsorted(jnp.cumsum(lengths), jnp.arange(rows * top), side="right").astype(jnp.int32)
    listing = items.reshape(top, rows).T
    listing = listing[jax.random.permutation(jax.random.fold_in(own, 1), rows)]
    turn = jax.random.randint(jax.random.fold_in(own, 2), (rows, 1), 0, top)
    return jnp.take_along_axis(listing, (jnp.arange(top)[None, :] + turn) % top, axis=1)


def portions_of(amount, total, bound, skew, full):
    loads = [(1 << 20) // math.isqrt(standing ** skew) + 1 for standing in range(1, amount + 1)]
    largest = bound if full else min(bound, max(-(-total // amount), total * loads[0] // sum(loads)))
    least = 1 if total - largest >= amount - 1 else 0
    given, rest = [largest] + [least] * (amount - 1), total - largest - least * (amount - 1)
    while rest > 0:
        movable = [i for i in range(1, amount) if given[i] < largest] or [i for i in range(1, amount) if given[i] < bound]
        mass, budget = sum([loads[i] for i in movable]), rest
        for i in movable:
            more = min(bound - given[i], max(1, budget * loads[i] // mass), rest)
            given[i] = given[i] + more
            rest = rest - more
    return np.array(given)


def noise(own_key, extent, scale, bound, cuts=(), kind=jnp.bfloat16):
    array = jax.random.normal(own_key, extent, jnp.float32) * scale
    if len(cuts) > 0:
        array = steps_of(own_key, extent, cuts, -0.22, 0.18) * array
    return jnp.clip(array, min=-bound, max=bound).astype(kind)


def bell_draw_with(own_key, dims, scale, most, cuts, heavy, kind=jnp.bfloat16):
    result = scale * jax.random.normal(own_key, dims, jnp.float32)
    if cuts:
        result = result * steps_of(own_key, dims, cuts, -0.22, 0.18)
    return jnp.clip(with_spikes(result, jax.random.fold_in(own_key, 3), *heavy), -most, most).astype(kind)


def setup_inputs(seed: int = 0) -> dict:
    seeds = jax.random.split(jax.random.key(seed), 18)
    stream = draw_stream(jax.random.fold_in(seeds[17], 71), 0)
    values_in = noise(seeds[1], (CW, TOKENS), 1.0, 6.0, ((0, 4), (1, 8)))
    in_gate = noise(seeds[2], (CW, TOKENS), 1.0, 6.0, ((0, 4), (1, 8)))
    out_gate = noise(seeds[3], (CW, TOKENS), 1.0, 6.0, ((0, 4), (1, 8)))
    documents = jnp.searchsorted(jnp.cumsum(uneven_parts(seeds[4], 2 * N_SP, TOKENS, 2 * TOK_DEV, 1)), jnp.arange(TOKENS), side="right").astype(jnp.int32)
    conv_taps = noise(seeds[5], (3, CW), 3 ** -0.5, 3.5, ((1, 4),), jnp.float32)
    head_gain = jnp.clip(1.0 + 0.18 * jax.random.normal(seeds[6], (CW,), jnp.float32), 0.1, 1.9)
    mix_weight = bell_draw_with(seeds[7], (CW, D), CW ** -0.5, 0.25, ((0, 4),), (0, 1, 4, 2.0))
    norm_gain = jnp.clip(1.0 + 0.18 * jax.random.normal(seeds[8], (D,), jnp.float32), 0.1, 1.9)
    routes_keys = jax.random.split(jax.random.fold_in(seeds[9], 1), TOKENS // TOK_DEV)
    routes_turns = jax.random.permutation(jax.random.fold_in(seeds[9], 3), TOKENS // TOK_DEV)
    routes = jax.vmap(lambda own, number: deal_out(jax.random.fold_in(seeds[9], 2), own, number, TOK_DEV, EXPERTS, TOP_K, CAP, 1))(routes_keys, routes_turns).reshape((TOKENS, TOP_K))
    route_weight = jnp.clip(0.2 + 0.8 * jax.random.uniform(seeds[10], (TOKENS, TOP_K), jnp.float32) ** steps_of(seeds[10], (TOKENS, TOP_K), ((0, 8),), -0.2, 0.2), 0.2, 1.0)
    expert_gate = noise(seeds[11], (EXPERTS, D, FE), D ** -0.5, 0.125, ((0, 8), (2, 4)))
    expert_up = noise(seeds[12], (EXPERTS, D, FE), D ** -0.5, 0.125, ((0, 8), (2, 4)))
    expert_down = noise(seeds[13], (EXPERTS, FE, D), FE ** -0.5, 0.125, ((0, 8), (2, 4)))
    shared_gate = noise(seeds[14], (D, FS), D ** -0.5, 0.125, ((1, 4),))
    shared_up = noise(seeds[15], (D, FS), D ** -0.5, 0.125, ((1, 4),))
    shared_down = bell_draw_with(seeds[16], (FS, D), FS ** -0.5, 0.1875, ((0, 4),), (0, 1, 4, 2.0))
    return {"stream": stream, "values_in": values_in, "in_gate": in_gate, "out_gate": out_gate, "documents": documents, "conv_taps": conv_taps, "head_gain": head_gain, "mix_weight": mix_weight, "norm_gain": norm_gain, "routes": routes, "route_weight": route_weight, "expert_gate": expert_gate, "expert_up": expert_up, "expert_down": expert_down, "shared_gate": shared_gate, "shared_up": shared_up, "shared_down": shared_down}


epsilon = 1e-06

def rounded(value):
    return lax.optimization_barrier(value.astype(jnp.bfloat16)).astype(jnp.float32)

def block_sum(left, right, parts):
    width = left.shape[1] // parts
    running = jnp.zeros((left.shape[0], right.shape[1]), jnp.float32)
    for block in range(parts):
        term = jnp.dot(left[:, block * width:(block + 1) * width], right[block * width:(block + 1) * width], preferred_element_type=jnp.float32)
        running = running + rounded(term)
    return running

def reference(stream, values_in, in_gate, out_gate, documents, conv_taps, head_gain, mix_weight, norm_gain, routes, route_weight, expert_gate, expert_up, expert_down, shared_gate, shared_up, shared_down):
    product = values_in.astype(jnp.float32) * in_gate.astype(jnp.float32)
    length = product.shape[1]
    padded = jnp.pad(product, ((0, 0), (2, 0)))
    doc_ids = jnp.pad(documents, (2, 0), constant_values=-1)
    convolved = jnp.zeros(product.shape, jnp.float32)
    for offset in range(3):
        same_doc = (doc_ids[offset:offset + length] == documents).astype(jnp.float32)
        convolved = convolved + conv_taps[offset][:, None] * padded[:, offset:offset + length] * same_doc[None, :]
    mixed = out_gate.astype(jnp.float32) * convolved
    heads = mixed.reshape(HEADS, HEAD, length)
    heads = heads * lax.rsqrt(lax.optimization_barrier(jnp.mean(heads * heads, axis=1, keepdims=True)) + epsilon)
    normed_heads = (heads.reshape(CW, length) * head_gain[:, None]).astype(jnp.bfloat16)
    mixer = block_sum(normed_heads.T, mix_weight, N_TP)
    hidden_state = stream.astype(jnp.float32).T + mixer
    normed = (hidden_state * lax.rsqrt(lax.optimization_barrier(jnp.mean(hidden_state * hidden_state, axis=1, keepdims=True)) + epsilon) * norm_gain[None, :]).astype(jnp.bfloat16)
    shared_mid = (jax.nn.silu(jnp.dot(normed, shared_gate, preferred_element_type=jnp.float32)) * jnp.dot(normed, shared_up, preferred_element_type=jnp.float32)).astype(jnp.bfloat16)
    shared = block_sum(shared_mid, shared_down, N_TP)
    groups = TOKENS // TOK_DEV
    flat_routes = routes.reshape(groups, TOK_DEV * TOP_K)
    onehot = (flat_routes[:, :, None] == jnp.arange(EXPERTS, dtype=jnp.int32)[None, None, :]).astype(jnp.int32)
    earlier = jnp.cumsum(onehot, axis=1) - onehot
    slot = lax.optimization_barrier(jnp.sum(earlier * onehot, axis=2))
    column = (jnp.arange(groups, dtype=jnp.int32)[:, None] * CAP + slot).reshape(-1).astype(jnp.int32)
    owner = (jnp.arange(TOKENS * TOP_K, dtype=jnp.int32) // TOP_K).astype(jnp.int32)
    chosen = flat_routes.reshape(-1)
    table = jnp.zeros((EXPERTS, groups * CAP), jnp.int32).at[chosen, column].set(owner)
    filled = jnp.zeros((EXPERTS, groups * CAP), jnp.bfloat16).at[chosen, column].set(1.0)

    def expert(number):
        rows = normed[table[number]] * filled[number][:, None]
        gate = jnp.dot(rows, expert_gate[number], preferred_element_type=jnp.float32)
        upward = jnp.dot(rows, expert_up[number], preferred_element_type=jnp.float32)
        middle = (jax.nn.silu(gate) * upward).astype(jnp.bfloat16)
        return jnp.dot(middle, expert_down[number], preferred_element_type=jnp.float32).astype(jnp.bfloat16)
    outputs = lax.map(expert, jnp.arange(EXPERTS, dtype=jnp.int32))
    picked = outputs[chosen, column].astype(jnp.float32).reshape(TOKENS, TOP_K, D)
    routed = lax.optimization_barrier(jnp.sum(picked * route_weight[:, :, None], axis=1))
    return (hidden_state + shared + routed).astype(jnp.bfloat16).T
```

```python
import functools

import jax
import jax.numpy as jnp
from jax import lax
from jax.experimental import pallas as pl
from jax.experimental.pallas import tpu as pltpu
from jax.sharding import PartitionSpec as P

HEAD = 64
CORES = 2
SUB = 8
ALONG_Z = (1, 2, 3)
epsilon = 1e-06
MESH = pl.DeviceIdType.MESH
F32 = jnp.float32
BF16 = jnp.bfloat16


def flipped(index, mask):
    bit = 1
    out = index
    while bit <= mask:
        if mask & bit:
            out = out + bit - 2 * bit * lax.rem(lax.div(index, bit), 2)
        bit *= 2
    return out


def dot(left, right):
    return jnp.dot(left, right, preferred_element_type=F32)


def silu(value):
    return value / (1.0 + jnp.exp(-value))


def column_of(row, width):
    return jnp.broadcast_to(row, (width, row.shape[1])).T


def kernel(
    n_sp, n_tp, cap,
    stream, values_in, in_gate, out_gate, documents, conv_taps, head_gain, mix_weight,
    norm_gain, routes, route_weight, expert_gate, expert_up, expert_down,
    shared_gate, shared_up, shared_down,
    out,
    mix_w, gate_w, up_w, sgate_w, sup_w, sdown_w, down_w,
    tail_s, prev_r, prev_docs, mix_s, mix_r, hidden_v, x_all, ss_s, ss_r, meta_r,
    sh_s, sh_r, mid_all, acc_v, pr_s, pr_r, zr_s, zr_r,
    load_sem, halo_send, halo_recv, mix_send, mix_recv, ss_send, ss_recv,
    meta_send, meta_recv, x_recv, xs_tp, xs_z, xs_d, xs_n, xs_p, sh_send, sh_recv,
    mid_send, mid_recv, fwd_send, fwd_recv, pr_send, pr_recv, zr_send, zr_recv,
):
    sp = lax.axis_index("sp")
    tp = lax.axis_index("tp")
    z = lax.div(sp, CORES)
    core = lax.rem(sp, CORES)
    n_z = n_sp // CORES
    feats, pos = stream.shape
    chans = values_in.shape[0]
    width = feats * n_tp
    hid = gate_w.shape[1]
    partner = {"sp": z * CORES + 1 - core}
    peers = [flipped(tp, d) for d in range(1, n_tp)]
    square = n_tp == 4 and n_z > 1
    near = peers[:2] if square else peers
    along_z = [d for d in ALONG_Z if d < n_z] if square else []
    layers = [flipped(z, d) for d in range(n_z)]
    pending = []

    def send(src, dst, ssem, rsem, device):
        copy = pltpu.make_async_remote_copy(
            src_ref=src, dst_ref=dst, send_sem=ssem, recv_sem=rsem,
            device_id=device, device_id_type=MESH,
        )
        copy.start()
        pending.append(copy)

    def arrived(dst, rsem):
        pltpu.make_async_remote_copy(
            src_ref=dst, dst_ref=dst, send_sem=rsem, recv_sem=rsem,
            device_id=partner, device_id_type=MESH,
        ).wait_recv()

    loads = [
        pltpu.make_async_copy(src, dst, load_sem.at[i])
        for i, (src, dst) in enumerate([
            (mix_weight, mix_w), (shared_gate, sgate_w), (shared_up, sup_w),
            (shared_down, sdown_w), (expert_gate.at[0], gate_w), (expert_up.at[0], up_w),
            (expert_down.at[0], down_w),
        ])
    ]
    loads[0].start()

    barrier = pltpu.get_barrier_semaphore()
    for peer in peers:
        pl.semaphore_signal(barrier, inc=1, device_id={"tp": peer}, device_id_type=MESH)
    for d in range(1, n_sp):
        pl.semaphore_signal(
            barrier, inc=1, device_id={"sp": lax.rem(sp + d, n_sp)}, device_id_type=MESH
        )
    with jax.named_scope("barrier"):
        pl.semaphore_wait(barrier, n_tp - 1 + n_sp - 1)

    product = values_in[...].astype(F32) * in_gate[...].astype(F32)
    tail_s[...] = product.T[pos - SUB:, :]
    after = {"sp": lax.rem(sp + 1, n_sp)}
    send(tail_s, prev_r.at[pl.ds(pos - SUB, SUB)], halo_send.at[0], halo_recv.at[0], after)
    send(documents, prev_docs, halo_send.at[1], halo_recv.at[1], after)
    for load in loads[1:]:
        load.start()

    named = routes[...]
    weights = route_weight[...]
    meta_rows = meta_r.shape[1]
    at_row = lax.broadcasted_iota(jnp.int32, (meta_rows, pos), 0)
    table = jnp.zeros((meta_rows, pos), F32)
    for k in range(routes.shape[0]):
        table = table + jnp.where(at_row == named[k:k + 1, :], weights[k:k + 1, :], 0.0)
    taps = [column_of(conv_taps[j:j + 1, :], pos) for j in range(3)]
    stream_t = stream[...].astype(F32).T

    prev_r[: pos - SUB, :] = jnp.zeros((pos - SUB, chans), F32)
    with jax.named_scope("w_halo"):
        arrived(prev_r.at[pl.ds(pos - SUB, SUB)], halo_recv.at[0])
        arrived(prev_docs, halo_recv.at[1])
    before = prev_r[...].T
    docs = documents[...]
    docs_before = jnp.where(sp > 0, prev_docs[...], -1)
    lane_c = lax.broadcasted_iota(jnp.int32, (chans, pos), 1)
    lane_1 = lax.broadcasted_iota(jnp.int32, (1, pos), 1)
    convolved = taps[2] * product
    for shift in (1, 2):
        moved = jnp.where(lane_c < shift, pltpu.roll(before, shift, 1), pltpu.roll(product, shift, 1))
        ids = jnp.where(lane_1 < shift, pltpu.roll(docs_before, shift, 1), pltpu.roll(docs, shift, 1))
        convolved = convolved + jnp.where(ids == docs, taps[2 - shift] * moved, 0.0)
    mixed = out_gate[...].astype(F32) * convolved
    heads = mixed.reshape(chans // HEAD, HEAD, pos)
    heads = heads * lax.rsqrt(jnp.mean(heads * heads, axis=1, keepdims=True) + epsilon)
    heads_t = (heads.reshape(chans, pos).T * head_gain[...]).astype(BF16)

    loads[0].wait()
    for b, peer in enumerate(peers + [tp]):
        cols = pl.ds(pl.multiple_of(peer * feats, feats), feats)
        mix_s[b] = dot(heads_t, mix_w[:, cols]).astype(BF16)
        if b < n_tp - 1:
            send(mix_s.at[b], mix_r.at[b], mix_send.at[b], mix_recv.at[b], {"tp": peer})

    hidden = stream_t + mix_s[n_tp - 1].astype(F32)
    for b in range(n_tp - 1):
        with jax.named_scope(f"w_mix{b}"):
            arrived(mix_r.at[b], mix_recv.at[b])
        hidden = hidden + mix_r[b].astype(F32)
    hidden_v[...] = hidden
    x_all[sp, tp] = (hidden * norm_gain[...]).astype(BF16)
    squares = jnp.sum(hidden * hidden, axis=1, keepdims=True)
    row = jnp.broadcast_to(squares, (pos, pos)).T[:SUB]
    ss_s[...] = row
    for b, peer in enumerate(peers):
        send(ss_s, ss_r.at[b], ss_send.at[b], ss_recv.at[b], {"tp": peer})
    own = x_all.at[sp, tp]
    for b, peer in enumerate(peers):
        send(own, own, xs_tp.at[0, b], x_recv.at[sp, tp], {"tp": peer})
    for d in range(1, n_z):
        send(own, own, xs_z.at[d], x_recv.at[sp, tp], {"sp": layers[d] * CORES + core})
    send(own, own, xs_p.at[0, 0], x_recv.at[sp, tp], partner)

    for b in range(n_tp - 1):
        with jax.named_scope(f"w_ss{b}"):
            arrived(ss_r.at[b], ss_recv.at[b])
        row = row + ss_r[b]
    scale = lax.rsqrt(row[:1] / width + epsilon)
    meta_r[sp] = jnp.where(at_row == meta_rows - 1, scale, table)
    for d in range(1, n_sp):
        send(meta_r.at[sp], meta_r.at[sp], meta_send.at[d], meta_recv.at[sp],
             {"sp": lax.rem(sp + d, n_sp)})

    def to_partner(slot, b, group):
        block = x_all.at[group, peers[b]]
        with jax.named_scope(f"w_x{slot}_{b}"):
            arrived(block, x_recv.at[group, peers[b]])
        send(block, block, xs_p.at[slot, b + 1], x_recv.at[group, peers[b]], partner)

    def from_layer(d):
        group = layers[d] * CORES + core
        block = x_all.at[group, tp]
        with jax.named_scope(f"w_layer{d}"):
            arrived(block, x_recv.at[group, tp])
        for b, peer in enumerate([] if square and d == 1 else (near if d in along_z else peers)):
            send(block, block, xs_tp.at[d, b], x_recv.at[group, tp], {"tp": peer})
        send(block, block, xs_p.at[d, 0], x_recv.at[group, tp], partner)

    for b in range(n_tp - 1):
        to_partner(0, b, sp)
        if square and b < 2:
            block = x_all.at[sp, peers[b]]
            send(block, block, xs_n.at[b], x_recv.at[sp, peers[b]],
                 {"sp": layers[1] * CORES + core})
    if square:
        block = x_all.at[sp, peers[2]]
        for d in along_z:
            send(block, block, xs_d.at[d], x_recv.at[sp, peers[2]],
                 {"sp": layers[d] * CORES + core})
    if n_z > 1:
        from_layer(1)

    with jax.named_scope("w_load"):
        for i in (1, 2, 3):
            loads[i].wait()
    scale_own = column_of(scale, pos)[:, :1]
    gate = jnp.zeros((pos, hid), F32)
    upward = jnp.zeros((pos, hid), F32)
    for b in range(n_tp):
        block = x_all[sp, b]
        gate = gate + dot(block, sgate_w[b * feats:(b + 1) * feats, :])
        upward = upward + dot(block, sup_w[b * feats:(b + 1) * feats, :])
    shared_mid = (silu(gate * scale_own) * (upward * scale_own)).astype(BF16)
    for b, peer in enumerate(peers + [tp]):
        cols = pl.ds(pl.multiple_of(peer * feats, feats), feats)
        sh_s[b] = dot(shared_mid, sdown_w[:, cols]).astype(BF16)
        if b < n_tp - 1:
            send(sh_s.at[b], sh_r.at[b], sh_send.at[b], sh_recv.at[b], {"tp": peer})

    for d in range(2, n_z):
        from_layer(d)

    with jax.named_scope("w_load2"):
        for i in (4, 5, 6):
            loads[i].wait()

    at_a = lax.broadcasted_iota(jnp.int32, (pos, pos), 0)
    at_b = lax.broadcasted_iota(jnp.int32, (pos, pos), 1)
    earlier = jnp.where(at_a < at_b, 1.0, 0.0).astype(BF16)
    rank_row = lax.broadcasted_iota(jnp.int32, (cap, pos), 0).astype(F32)
    rank_lane = lax.broadcasted_iota(jnp.int32, (pos, cap), 1).astype(F32)

    def groups_of(d):
        return layers[d] * CORES + core, layers[d] * CORES + 1 - core

    def slots_of(group):
        weight = meta_r[group, pl.ds(sp, 1), :]
        mask = jnp.where(weight > 0.0, 1.0, 0.0)
        count = dot(jnp.broadcast_to(mask, (2 * SUB, pos)).astype(BF16), earlier)[:1]
        return weight, jnp.where(weight > 0.0, count, -1.0)

    def widen(d):
        mine, other = groups_of(d)
        if d > 0:
            for b in range(n_tp - 1):
                to_partner(d, b, mine)
            with jax.named_scope(f"w_meta{d}"):
                arrived(meta_r.at[mine], meta_recv.at[mine])
        with jax.named_scope(f"w_other{d}"):
            arrived(meta_r.at[other], meta_recv.at[other])
            for b in range(n_tp):
                arrived(x_all.at[other, b], x_recv.at[other, b])
        gate = jnp.zeros((CORES * pos, hid), F32)
        upward = jnp.zeros((CORES * pos, hid), F32)
        for b in range(n_tp):
            block = jnp.concatenate([x_all[mine, b], x_all[other, b]], axis=0)
            gate = gate + dot(block, gate_w[b * feats:(b + 1) * feats, :])
            upward = upward + dot(block, up_w[b * feats:(b + 1) * feats, :])
        scales = jnp.concatenate([
            column_of(meta_r[group, meta_rows - 1:, :], pos)[:, :1] for group in (mine, other)
        ], axis=0)
        middle = (silu(gate * scales) * (upward * scales)).astype(BF16)
        for i, group in enumerate((mine, other)):
            slot = slots_of(group)[1]
            pick = jnp.where(rank_row == slot, 1.0, 0.0).astype(BF16)
            mid_all[d, tp, i * cap:(i + 1) * cap, :] = dot(
                pick, middle[i * pos:(i + 1) * pos]
            ).astype(BF16)
        block = mid_all.at[d, tp]
        for b, peer in enumerate(near):
            send(block, block, mid_send.at[d, b], mid_recv.at[d, tp], {"tp": peer})

    def relay(d):
        for b, peer in enumerate(near):
            with jax.named_scope(f"w_mid{d}_{b}"):
                arrived(mid_all.at[d, peer], mid_recv.at[d, peer])
            if square:
                part = mid_all.at[d, peer, pl.ds(b * cap, cap)]
                send(part, part, fwd_send.at[d, b], fwd_recv.at[d, b], {"tp": near[1 - b]})

    def narrow(d):
        if square:
            for b in range(2):
                with jax.named_scope(f"w_fwd{d}_{b}"):
                    arrived(mid_all.at[d, peers[2], pl.ds(b * cap, cap)], fwd_recv.at[d, b])
        total = jnp.zeros((CORES * cap, feats), F32)
        for b in range(n_tp):
            total = total + dot(mid_all[d, b], down_w[b * hid:(b + 1) * hid, :])
        total = total.astype(BF16)
        terms = []
        for i, group in enumerate(groups_of(d)):
            weight, slot = slots_of(group)
            place = jnp.where(rank_lane == column_of(slot, cap), 1.0, 0.0).astype(BF16)
            term = dot(place, total[i * cap:(i + 1) * cap])
            terms.append(term * column_of(weight, pos)[:, :1])
        acc_v[d] = terms[0]
        pr_s[d] = terms[1].astype(BF16)
        send(pr_s.at[d], pr_r.at[d], pr_send.at[d], pr_recv.at[d], partner)

    def join(d):
        with jax.named_scope(f"w_pr{d}"):
            arrived(pr_r.at[d], pr_recv.at[d])
        if d > 0:
            zr_s[d] = (acc_v[d] + pr_r[d].astype(F32)).astype(BF16)
            send(zr_s.at[d], zr_r.at[d], zr_send.at[d], zr_recv.at[d],
                 {"sp": layers[d] * CORES + core})

    order = list(range(1, n_z)) + [0]
    for step in range(n_z + 3):
        for lag, stage in enumerate((widen, relay, narrow, join)):
            if 0 <= step - lag < n_z:
                stage(order[step - lag])

    result = hidden_v[...] + sh_s[n_tp - 1].astype(F32)
    for b in range(n_tp - 1):
        with jax.named_scope(f"w_sh{b}"):
            arrived(sh_r.at[b], sh_recv.at[b])
        result = result + sh_r[b].astype(F32)
    result = result + acc_v[0] + pr_r[0].astype(F32)
    for d in range(1, n_z):
        with jax.named_scope(f"w_zr{d}"):
            arrived(zr_r.at[d], zr_recv.at[d])
        result = result + zr_r[d].astype(F32)
    out[...] = result.T.astype(BF16)
    with jax.named_scope("w_send"):
        for copy in pending:
            copy.wait_send()


def local(n_sp, n_tp, *args):
    (stream, values_in, in_gate, out_gate, documents, conv_taps, head_gain, mix_weight,
     norm_gain, routes, route_weight, expert_gate, expert_up, expert_down,
     shared_gate, shared_up, shared_down) = args
    feats, pos = stream.shape
    chans = values_in.shape[0]
    width = feats * n_tp
    hid = expert_gate.shape[2]
    n_z = n_sp // CORES
    meta_rows = -(-(n_sp + 1) // SUB) * SUB
    experts = n_sp * expert_gate.shape[0]
    bound = 3 * pos * routes.shape[1] // (2 * experts)
    cap = -(-bound // (2 * SUB)) * 2 * SUB
    vmem = pl.BlockSpec(memory_space=pltpu.VMEM)
    anywhere = pl.BlockSpec(memory_space=pl.ANY)
    dma = pltpu.SemaphoreType.DMA
    scratch = [
        pltpu.VMEM((chans, width), BF16),
        pltpu.VMEM((width, hid), BF16),
        pltpu.VMEM((width, hid), BF16),
        pltpu.VMEM((width, hid), BF16),
        pltpu.VMEM((width, hid), BF16),
        pltpu.VMEM((hid, width), BF16),
        pltpu.VMEM((n_tp * hid, feats), BF16),
        pltpu.VMEM((SUB, chans), F32),
        pltpu.VMEM((pos, chans), F32),
        pltpu.VMEM((1, pos), jnp.int32),
        pltpu.VMEM((n_tp, pos, feats), BF16),
        pltpu.VMEM((n_tp, pos, feats), BF16),
        pltpu.VMEM((pos, feats), F32),
        pltpu.VMEM((n_sp, n_tp, pos, feats), BF16),
        pltpu.VMEM((SUB, pos), F32),
        pltpu.VMEM((n_tp, SUB, pos), F32),
        pltpu.VMEM((n_sp, meta_rows, pos), F32),
        pltpu.VMEM((n_tp, pos, feats), BF16),
        pltpu.VMEM((n_tp, pos, feats), BF16),
        pltpu.VMEM((n_z, n_tp, CORES * cap, hid), BF16),
        pltpu.VMEM((n_z, pos, feats), F32),
        pltpu.VMEM((n_z, pos, feats), BF16),
        pltpu.VMEM((n_z, pos, feats), BF16),
        pltpu.VMEM((n_z, pos, feats), BF16),
        pltpu.VMEM((n_z, pos, feats), BF16),
        dma((7,)),
        dma((2,)), dma((2,)),
        dma((n_tp,)), dma((n_tp,)),
        dma((n_tp,)), dma((n_tp,)),
        dma((n_sp,)), dma((n_sp,)),
        dma((n_sp, n_tp)),
        dma((n_z, n_tp)), dma((n_z,)), dma((n_z,)), dma((n_tp,)), dma((n_z, n_tp)),
        dma((n_tp,)), dma((n_tp,)),
        dma((n_z, n_tp)), dma((n_z, n_tp)),
        dma((n_z, 2)), dma((n_z, 2)),
        dma((n_z,)), dma((n_z,)),
        dma((n_z,)), dma((n_z,)),
    ]
    return pl.pallas_call(
        functools.partial(kernel, n_sp, n_tp, cap),
        out_shape=jax.ShapeDtypeStruct((feats, pos), BF16),
        in_specs=[vmem] * 7 + [anywhere] + [vmem] * 3 + [anywhere] * 6,
        out_specs=vmem,
        scratch_shapes=scratch,
        compiler_params=pltpu.CompilerParams(
            collective_id=0, has_side_effects=True, vmem_limit_bytes=64 * 1024 * 1024 - 65536
        ),
    )(
        stream, values_in, in_gate, out_gate, documents.reshape(1, pos), conv_taps,
        head_gain.reshape(1, chans), mix_weight, norm_gain.reshape(1, feats), routes.T,
        route_weight.T, expert_gate, expert_up, expert_down, shared_gate, shared_up, shared_down,
    )


def solution(mesh):
    in_specs = (
        P("tp", "sp"),
        P("tp", "sp"),
        P("tp", "sp"),
        P("tp", "sp"),
        P("sp"),
        P(None, "tp"),
        P("tp"),
        P("tp", None),
        P("tp"),
        P("sp", None),
        P("sp", None),
        P("sp", None, "tp"),
        P("sp", None, "tp"),
        P("sp", None, "tp"),
        P(None, "tp"),
        P(None, "tp"),
        P("tp", None),
    )
    body = functools.partial(local, mesh.shape["sp"], mesh.shape["tp"])
    return jax.shard_map(
        body, mesh=mesh, in_specs=in_specs, out_specs=P("tp", "sp"), check_vma=False
    )
```

```python
import functools

import jax
import jax.numpy as jnp
from jax import lax
from jax.experimental import pallas as pl
from jax.experimental.pallas import tpu as pltpu
from jax.sharding import PartitionSpec as P

HEAD = 64
CORES = 2
SUB = 8
EDGE = 16
epsilon = 1e-06
MESH = pl.DeviceIdType.MESH
F32 = jnp.float32
BF16 = jnp.bfloat16


def flipped(index, mask):
    bit = 1
    out = index
    while bit <= mask:
        if mask & bit:
            out = out + bit - 2 * bit * lax.rem(lax.div(index, bit), 2)
        bit *= 2
    return out


def dot(left, right):
    return jnp.dot(left, right, preferred_element_type=F32)


def silu(value):
    return value / (1.0 + jnp.exp(-value))


def column_of(row, width):
    return jnp.broadcast_to(row, (width, row.shape[1])).T


def kernel(
    n_sp, n_tp, cap,
    stream_h, values_h, in_h, out_h, documents_h, taps_h, head_h, mix_weight,
    norm_h, routes_h, route_weight_h, expert_gate, expert_up, expert_down,
    shared_gate, shared_up, shared_down,
    out,
    stream, values_in, in_gate, out_gate, documents, conv_taps, head_gain,
    norm_gain, routes, route_weight, mix_w, gate_w, up_w, sgate_w, sup_w, sdown_w, down_w,
    tail_s, prev_r, prev_docs, mix_s, mix_r, hidden_v, x_all, ss_s, ss_r, meta_r,
    sh_s, sh_r, mid_all, acc_v, pr_s, pr_r, zr_s, zr_r,
    small_sem, load_sem, halo_send, halo_recv, mix_send, mix_recv, ss_send, ss_recv,
    meta_send, meta_recv, x_recv, xs_tp, xs_z, xs_r, xs_n, xs_p, sh_send, sh_recv,
    mid_send, mid_recv, fwd_send, fwd_recv, pr_send, pr_recv, zr_send, zr_recv,
):
    sp = lax.axis_index("sp")
    tp = lax.axis_index("tp")
    z = lax.div(sp, CORES)
    core = lax.rem(sp, CORES)
    n_z = n_sp // CORES
    feats, pos = stream.shape
    chans = values_in.shape[0]
    width = feats * n_tp
    hid = gate_w.shape[1]
    partner = {"sp": z * CORES + 1 - core}
    peers = [flipped(tp, d) for d in range(1, n_tp)]
    square = n_tp == 4 and n_z == 4
    near = peers[:2] if square else peers
    layers = [flipped(z, d) for d in range(n_z)]
    pending = []
    inner = lax.div(z + 1, 2) == 1
    if square:
        layers[2:] = [jnp.where(inner, layers[3], layers[2]), jnp.where(inner, layers[2], layers[3])]
    turns = {"inner": [], "end": []}

    def only(where, stage, *args):
        @pl.when(inner if where == "inner" else jnp.logical_not(inner))
        def _():
            kept = len(pending)
            stage(*args)
            turns[where].extend((sem, size) for _, sem, size in pending[kept:])
            del pending[kept:]

    def onward(block, rsem, slot, d):
        def relay_on():
            send(block, block, (xs_r, slot, d), rsem, {"sp": layers[2 if d < 2 else 1] * CORES + core})
        return relay_on

    def send(src, dst, ssem, rsem, device):
        sem = ssem[0].at[ssem[1:]] if isinstance(ssem, tuple) else ssem
        copy = pltpu.make_async_remote_copy(
            src_ref=src, dst_ref=dst, send_sem=sem, recv_sem=rsem,
            device_id=device, device_id_type=MESH,
        )
        copy.start()
        pending.append((copy, ssem, src.shape))

    def arrived(dst, rsem):
        pltpu.make_async_remote_copy(
            src_ref=dst, dst_ref=dst, send_sem=rsem, recv_sem=rsem,
            device_id=partner, device_id_type=MESH,
        ).wait_recv()

    loads = [
        pltpu.make_async_copy(src, dst, load_sem.at[i])
        for i, (src, dst) in enumerate([
            (mix_weight, mix_w), (shared_gate, sgate_w), (shared_up, sup_w),
            (shared_down, sdown_w), (expert_gate.at[0], gate_w), (expert_up.at[0], up_w),
            (expert_down.at[0], down_w),
        ])
    ]
    smalls = [
        pltpu.make_async_copy(src, dst, small_sem.at[i])
        for i, (src, dst) in enumerate([
            (values_h, values_in), (in_h, in_gate), (documents_h, documents), (out_h, out_gate),
            (taps_h, conv_taps), (head_h, head_gain), (routes_h, routes),
            (route_weight_h, route_weight), (stream_h, stream), (norm_h, norm_gain),
        ])
    ]

    barrier = pltpu.get_barrier_semaphore()
    for peer in peers:
        pl.semaphore_signal(barrier, inc=1, device_id={"tp": peer}, device_id_type=MESH)
    for d in range(1, n_sp):
        pl.semaphore_signal(
            barrier, inc=1, device_id={"sp": lax.rem(sp + d, n_sp)}, device_id_type=MESH
        )
    for copy in smalls:
        copy.start()
    loads[0].start()
    for copy in smalls[:3]:
        copy.wait()
    product = values_in[...].astype(F32) * in_gate[...].astype(F32)
    tail_s[...] = product.T[pos - SUB:, :]
    for copy in smalls[3:]:
        copy.wait()

    tap_rows = jnp.concatenate([conv_taps[...], jnp.zeros((SUB - 3, chans), F32)], axis=0).T
    taps = [jnp.broadcast_to(tap_rows[:, j:j + 1], (chans, pos)) for j in range(3)]
    docs = documents[...]
    lane_c = lax.broadcasted_iota(jnp.int32, (chans, pos), 1)
    lane_1 = lax.broadcasted_iota(jnp.int32, (1, pos), 1)

    def heads_of(before, docs_before):
        convolved = taps[2] * product
        for shift in (1, 2):
            moved = pltpu.roll(product, shift, 1)
            if before is not None:
                moved = jnp.where(lane_c < shift, pltpu.roll(before, shift, 1), moved)
            ids = jnp.where(lane_1 < shift, pltpu.roll(docs_before, shift, 1), pltpu.roll(docs, shift, 1))
            convolved = convolved + jnp.where(ids == docs, taps[2 - shift] * moved, 0.0)
        mixed = out_gate[...].astype(F32) * convolved
        heads = mixed.reshape(chans // HEAD, HEAD, pos)
        heads = heads * lax.rsqrt(jnp.mean(heads * heads, axis=1, keepdims=True) + epsilon)
        return (heads.reshape(chans, pos).T * head_gain[...]).astype(BF16)

    def mix(rows, heads_t):
        for b, peer in enumerate(peers + [tp]):
            cols = pl.ds(pl.multiple_of(peer * feats, feats), feats)
            mix_s[b, rows[0]:rows[1]] = dot(heads_t[rows[0]:rows[1]], mix_w[:, cols]).astype(BF16)

    def send_mix(rows, stage):
        part = pl.ds(rows[0], rows[1] - rows[0])
        for b, peer in enumerate(peers):
            send(mix_s.at[b, part], mix_r.at[b, part], mix_send.at[stage, b],
                 mix_recv.at[stage, b], {"tp": peer})

    heads_t = heads_of(None, jnp.full((1, pos), -1, jnp.int32))
    loads[0].wait()
    for load in loads[1:]:
        load.start()
    mix((EDGE, pos), heads_t)
    with jax.named_scope("barrier"):
        pl.semaphore_wait(barrier, n_tp - 1 + n_sp - 1)
    after = {"sp": lax.rem(sp + 1, n_sp)}
    halo = [
        pltpu.make_async_remote_copy(
            src_ref=src, dst_ref=dst, send_sem=halo_send.at[i], recv_sem=halo_recv.at[i],
            device_id=after, device_id_type=MESH,
        )
        for i, (src, dst) in enumerate([
            (tail_s, prev_r.at[pl.ds(pos - SUB, SUB)]), (documents, prev_docs),
        ])
    ]

    @pl.when(sp < n_sp - 1)
    def _():
        for copy in halo:
            copy.start()

    send_mix((EDGE, pos), 0)

    @pl.when(sp == 0)
    def _():
        prev_r[...] = jnp.zeros((pos, chans), F32)
        prev_docs[...] = jnp.full((1, pos), -1, jnp.int32)

    @pl.when(sp > 0)
    def _():
        prev_r[: pos - SUB, :] = jnp.zeros((pos - SUB, chans), F32)
        with jax.named_scope("w_halo"):
            for copy in halo:
                copy.wait_recv()

    heads_t = heads_of(prev_r[...].T, prev_docs[...])
    mix((0, EDGE), heads_t)
    send_mix((0, EDGE), 1)

    named = routes[...]
    weights = route_weight[...]
    meta_rows = meta_r.shape[1]
    at_row = lax.broadcasted_iota(jnp.int32, (meta_rows, pos), 0)
    table = jnp.zeros((meta_rows, pos), F32)
    for k in range(routes.shape[0]):
        table = table + jnp.where(at_row == named[k:k + 1, :], weights[k:k + 1, :], 0.0)
    stream_t = stream[...].astype(F32).T

    hidden = stream_t + mix_s[n_tp - 1].astype(F32)
    for b in range(n_tp - 1):
        with jax.named_scope(f"w_mix{b}"):
            arrived(mix_r.at[b, pl.ds(EDGE, pos - EDGE)], mix_recv.at[0, b])
            arrived(mix_r.at[b, pl.ds(0, EDGE)], mix_recv.at[1, b])
        hidden = hidden + mix_r[b].astype(F32)
    hidden_v[...] = hidden
    x_all[sp, tp] = (hidden * norm_gain[...]).astype(BF16)
    squares = jnp.sum(hidden * hidden, axis=1, keepdims=True)
    row = jnp.broadcast_to(squares, (pos, pos)).T[:SUB]
    ss_s[...] = row
    for b, peer in enumerate(peers):
        send(ss_s, ss_r.at[b], ss_send.at[b], ss_recv.at[b], {"tp": peer})
    own = x_all.at[sp, tp]
    for b, peer in enumerate(peers):
        send(own, own, (xs_tp, 0, b), x_recv.at[sp, tp], {"tp": peer})
    for d in ([1] if square else range(1, n_z)):
        send(own, own, (xs_z, d), x_recv.at[sp, tp], {"sp": layers[d] * CORES + core})
    if square:
        only("inner", onward(own, x_recv.at[sp, tp], 0, 0))
    send(own, own, (xs_p, 0, 0), x_recv.at[sp, tp], partner)

    for b in range(n_tp - 1):
        with jax.named_scope(f"w_ss{b}"):
            arrived(ss_r.at[b], ss_recv.at[b])
        row = row + ss_r[b]
    scale = lax.rsqrt(row[:1] / width + epsilon)
    meta_r[sp] = jnp.where(at_row == meta_rows - 1, scale, table)
    for d in range(1, n_sp):
        send(meta_r.at[sp], meta_r.at[sp], meta_send.at[d], meta_recv.at[sp],
             {"sp": lax.rem(sp + d, n_sp)})

    def to_partner(slot, b, group):
        block = x_all.at[group, peers[b]]
        with jax.named_scope(f"w_x{slot}_{b}"):
            arrived(block, x_recv.at[group, peers[b]])
        send(block, block, (xs_p, slot, b + 1), x_recv.at[group, peers[b]], partner)

    def from_layer(d):
        group = layers[d] * CORES + core
        block = x_all.at[group, tp]
        with jax.named_scope(f"w_layer{d}"):
            arrived(block, x_recv.at[group, tp])
        for b, peer in enumerate([] if square and d != 2 else near):
            send(block, block, (xs_tp, d, b), x_recv.at[group, tp], {"tp": peer})
        send(block, block, (xs_p, d, 0), x_recv.at[group, tp], partner)

    def closer(b):
        block = x_all.at[sp, peers[b]]
        send(block, block, (xs_n, b), x_recv.at[sp, peers[b]], {"sp": layers[1] * CORES + core})

    def from_layer_inner(d):
        group = layers[d] * CORES + core
        from_layer(d)
        onward(x_all.at[group, tp], x_recv.at[group, tp], 0, d)()

    if square:
        only("inner", from_layer_inner, 1)
        only("inner", from_layer_inner, 2)

    with jax.named_scope("w_load"):
        for i in (1, 2, 3):
            loads[i].wait()
    scale_own = column_of(scale, pos)[:, :1]

    def shared_part(peer):
        rows = pl.ds(pl.multiple_of(peer * feats, feats), feats)
        block = x_all[sp, peer]
        return dot(block, sgate_w[rows, :]), dot(block, sup_w[rows, :])

    gate, upward = shared_part(tp)
    for b in range(n_tp - 1):
        to_partner(0, b, sp)
        block = x_all.at[sp, peers[b]]
        if square:
            closer(b)
        if square and b == 2:
            only("inner", onward(block, x_recv.at[sp, peers[2]], 3, 0))
        more = shared_part(peers[b])
        gate, upward = gate + more[0], upward + more[1]
    shared_mid = (silu(gate * scale_own) * (upward * scale_own)).astype(BF16)
    for b, peer in enumerate(peers + [tp]):
        cols = pl.ds(pl.multiple_of(peer * feats, feats), feats)
        sh_s[b] = dot(shared_mid, sdown_w[:, cols]).astype(BF16)
        if b < n_tp - 1:
            send(sh_s.at[b], sh_r.at[b], sh_send.at[b], sh_recv.at[b], {"tp": peer})

    with jax.named_scope("w_load2"):
        for i in (4, 5, 6):
            loads[i].wait()

    at_a = lax.broadcasted_iota(jnp.int32, (pos, pos), 0)
    at_b = lax.broadcasted_iota(jnp.int32, (pos, pos), 1)
    earlier = jnp.where(at_a < at_b, 1.0, 0.0).astype(BF16)
    rank_row = lax.broadcasted_iota(jnp.int32, (cap, pos), 0).astype(F32)
    rank_lane = lax.broadcasted_iota(jnp.int32, (pos, cap), 1).astype(F32)

    def groups_of(d):
        return layers[d] * CORES + core, layers[d] * CORES + 1 - core

    def slots_of(group):
        weight = meta_r[group, pl.ds(sp, 1), :]
        mask = jnp.where(weight > 0.0, 1.0, 0.0)
        count = dot(jnp.broadcast_to(mask, (2 * SUB, pos)).astype(BF16), earlier)[:1]
        return weight, jnp.where(weight > 0.0, count, -1.0)

    def fetch(d, b):
        to_partner(d, b, groups_of(d)[0])

    def fetch_inner(d, b):
        group = groups_of(d)[0]
        to_partner(d, b, group)
        block = x_all.at[group, peers[b]]
        onward(block, x_recv.at[group, peers[b]], b + 1, d)()

    def widen(d):
        mine, other = groups_of(d)
        with jax.named_scope(f"w_other{d}"):
            if d > 0:
                arrived(meta_r.at[mine], meta_recv.at[mine])
            arrived(meta_r.at[other], meta_recv.at[other])
            for b in range(n_tp):
                arrived(x_all.at[other, b], x_recv.at[other, b])
        gate = jnp.zeros((CORES * pos, hid), F32)
        upward = jnp.zeros((CORES * pos, hid), F32)
        for b in range(n_tp):
            block = jnp.concatenate([x_all[mine, b], x_all[other, b]], axis=0)
            gate = gate + dot(block, gate_w[b * feats:(b + 1) * feats, :])
            upward = upward + dot(block, up_w[b * feats:(b + 1) * feats, :])
        scales = jnp.concatenate([
            column_of(meta_r[group, meta_rows - 1:, :], pos)[:, :1] for group in (mine, other)
        ], axis=0)
        middle = (silu(gate * scales) * (upward * scales)).astype(BF16)
        for i, group in enumerate((mine, other)):
            slot = slots_of(group)[1]
            pick = jnp.where(rank_row == slot, 1.0, 0.0).astype(BF16)
            mid_all[d, tp, i * cap:(i + 1) * cap, :] = dot(
                pick, middle[i * pos:(i + 1) * pos]
            ).astype(BF16)

    def mids(d, i):
        block = mid_all.at[d, tp, pl.ds(i * cap, cap)]
        for b, peer in enumerate(near):
            send(block, block, (mid_send, d, i, b), mid_recv.at[d, i, tp], {"tp": peer})

    def relay(d, i):
        for b, peer in enumerate(near):
            part = mid_all.at[d, peer, pl.ds(i * cap, cap)]
            with jax.named_scope(f"w_mid{d}_{i}_{b}"):
                arrived(part, mid_recv.at[d, i, peer])
            if square and b == i:
                send(part, part, (fwd_send, d, i), fwd_recv.at[d, i], {"tp": near[1 - b]})

    def narrow(d):
        if square:
            for b in range(2):
                with jax.named_scope(f"w_fwd{d}_{b}"):
                    arrived(mid_all.at[d, peers[2], pl.ds(b * cap, cap)], fwd_recv.at[d, b])
        total = jnp.zeros((CORES * cap, feats), F32)
        for b in range(n_tp):
            total = total + dot(mid_all[d, b], down_w[b * hid:(b + 1) * hid, :])
        total = total.astype(BF16)
        terms = []
        for i, group in enumerate(groups_of(d)):
            weight, slot = slots_of(group)
            place = jnp.where(rank_lane == column_of(slot, cap), 1.0, 0.0).astype(BF16)
            term = dot(place, total[i * cap:(i + 1) * cap])
            terms.append(term * column_of(weight, pos)[:, :1])
        acc_v[d] = terms[0]
        pr_s[d] = terms[1].astype(BF16)
        send(pr_s.at[d], pr_r.at[d], (pr_send, d), pr_recv.at[d], partner)

    def join(d):
        with jax.named_scope(f"w_pr{d}"):
            arrived(pr_r.at[d], pr_recv.at[d])
        if d > 0:
            zr_s[d] = (acc_v[d] + pr_r[d].astype(F32)).astype(BF16)
            send(zr_s.at[d], zr_r.at[z], (zr_send, d), zr_recv.at[z],
                 {"sp": layers[d] * CORES + core})

    def run(plan):
        for stage, *where in plan:
            stage(*where)

    if square:
        plan = [(from_layer, 1), (widen, 0), (mids, 0, 0), (from_layer, 2), (mids, 0, 1)]
        plan += [(fetch, 1, b) for b in range(3)] + [(widen, 1), (mids, 1, 0), (mids, 1, 1)]
        plan += [(relay, 0, 0), (relay, 0, 1), (from_layer, 3)]
        plan += [(fetch, 2, b) for b in range(3)] + [(widen, 2), (mids, 2, 0), (mids, 2, 1)]
        plan += [(relay, 1, 0), (relay, 1, 1), (relay, 2, 0)]
        plan += [(fetch, 3, b) for b in range(3)] + [(widen, 3), (mids, 3, 0), (mids, 3, 1)]
        plan += [(relay, 2, 1), (narrow, 1), (relay, 3, 0), (join, 1), (relay, 3, 1)]
        plan += [(narrow, 2), (join, 2), (narrow, 0), (narrow, 3), (join, 3), (join, 0)]
        only("end", run, plan)
        plan = [(from_layer_inner, 3), (widen, 0), (mids, 0, 0), (fetch_inner, 2, 2)]
        plan += [(fetch_inner, 1, b) for b in range(3)] + [(fetch, 2, 0), (fetch, 2, 1)]
        plan += [(widen, 1), (mids, 1, 0), (mids, 1, 1), (widen, 2), (mids, 2, 0), (mids, 2, 1)]
        plan += [(relay, 0, 0)] + [(fetch_inner, 3, b) for b in range(3)] + [(widen, 3)]
        plan += [(relay, 1, 0), (relay, 1, 1), (mids, 3, 0), (mids, 3, 1), (relay, 2, 0), (relay, 2, 1)]
        plan += [(mids, 0, 1), (narrow, 1), (relay, 3, 0), (relay, 3, 1), (join, 1), (narrow, 2)]
        plan += [(relay, 0, 1), (join, 2), (narrow, 3), (join, 3), (narrow, 0), (join, 0)]
        only("inner", run, plan)
    else:
        plan = [(from_layer, d) for d in range(1, n_z)]
        for d in range(n_z):
            plan += [(fetch, d, b) for b in range(n_tp - 1)] if d else []
            plan += [(widen, d), (mids, d, 0), (mids, d, 1)]
        for d in range(n_z):
            plan += [(relay, d, 0), (relay, d, 1), (narrow, d), (join, d)]
        run(plan)

    result = hidden_v[...] + sh_s[n_tp - 1].astype(F32)
    for b in range(n_tp - 1):
        with jax.named_scope(f"w_sh{b}"):
            arrived(sh_r.at[b], sh_recv.at[b])
        result = result + sh_r[b].astype(F32)
    result = result + acc_v[0] + pr_r[0].astype(F32)
    for d in range(1, n_z):
        with jax.named_scope(f"w_zr{d}"):
            arrived(zr_r.at[layers[d]], zr_recv.at[layers[d]])
        result = result + zr_r[layers[d]].astype(F32)
    out[...] = result.T.astype(BF16)
    with jax.named_scope("w_send"):
        for copy, *_ in pending:
            copy.wait_send()

        @pl.when(sp < n_sp - 1)
        def _():
            for copy in halo:
                copy.wait_send()

        def sent(sems):
            for sem, size in sems:
                like = own if size == (pos, feats) else mid_all.at[0, 0, pl.ds(0, size[0])]
                pltpu.make_async_remote_copy(
                    src_ref=like, dst_ref=like, send_sem=sem[0].at[sem[1:]],
                    recv_sem=sem[0].at[sem[1:]], device_id=partner, device_id_type=MESH,
                ).wait_send()

        for where, sems in turns.items():
            if sems:
                only(where, sent, list(sems))


def local(n_sp, n_tp, *args):
    (stream, values_in, in_gate, out_gate, documents, conv_taps, head_gain, mix_weight,
     norm_gain, routes, route_weight, expert_gate, expert_up, expert_down,
     shared_gate, shared_up, shared_down) = args
    feats, pos = stream.shape
    chans = values_in.shape[0]
    width = feats * n_tp
    hid = expert_gate.shape[2]
    n_z = n_sp // CORES
    meta_rows = -(-(n_sp + 1) // SUB) * SUB
    experts = n_sp * expert_gate.shape[0]
    bound = 3 * pos * routes.shape[1] // (2 * experts)
    cap = -(-bound // (2 * SUB)) * 2 * SUB
    vmem = pl.BlockSpec(memory_space=pltpu.VMEM)
    anywhere = pl.BlockSpec(memory_space=pl.ANY)
    dma = pltpu.SemaphoreType.DMA
    scratch = [
        pltpu.VMEM((feats, pos), BF16),
        pltpu.VMEM((chans, pos), BF16),
        pltpu.VMEM((chans, pos), BF16),
        pltpu.VMEM((chans, pos), BF16),
        pltpu.VMEM((1, pos), jnp.int32),
        pltpu.VMEM(conv_taps.shape, F32),
        pltpu.VMEM((1, chans), F32),
        pltpu.VMEM((1, feats), F32),
        pltpu.VMEM((routes.shape[1], pos), jnp.int32),
        pltpu.VMEM((routes.shape[1], pos), F32),
        pltpu.VMEM((chans, width), BF16),
        pltpu.VMEM((width, hid), BF16),
        pltpu.VMEM((width, hid), BF16),
        pltpu.VMEM((width, hid), BF16),
        pltpu.VMEM((width, hid), BF16),
        pltpu.VMEM((hid, width), BF16),
        pltpu.VMEM((n_tp * hid, feats), BF16),
        pltpu.VMEM((SUB, chans), F32),
        pltpu.VMEM((pos, chans), F32),
        pltpu.VMEM((1, pos), jnp.int32),
        pltpu.VMEM((n_tp, pos, feats), BF16),
        pltpu.VMEM((n_tp, pos, feats), BF16),
        pltpu.VMEM((pos, feats), F32),
        pltpu.VMEM((n_sp, n_tp, pos, feats), BF16),
        pltpu.VMEM((SUB, pos), F32),
        pltpu.VMEM((n_tp, SUB, pos), F32),
        pltpu.VMEM((n_sp, meta_rows, pos), F32),
        pltpu.VMEM((n_tp, pos, feats), BF16),
        pltpu.VMEM((n_tp, pos, feats), BF16),
        pltpu.VMEM((n_z, n_tp, CORES * cap, hid), BF16),
        pltpu.VMEM((n_z, pos, feats), F32),
        pltpu.VMEM((n_z, pos, feats), BF16),
        pltpu.VMEM((n_z, pos, feats), BF16),
        pltpu.VMEM((n_z, pos, feats), BF16),
        pltpu.VMEM((n_z, pos, feats), BF16),
        dma((10,)), dma((7,)),
        dma((2,)), dma((2,)),
        dma((2, n_tp)), dma((2, n_tp)),
        dma((n_tp,)), dma((n_tp,)),
        dma((n_sp,)), dma((n_sp,)),
        dma((n_sp, n_tp)),
        dma((n_z, n_tp)), dma((n_z,)), dma((4, n_z)), dma((n_tp,)), dma((n_z, n_tp)),
        dma((n_tp,)), dma((n_tp,)),
        dma((n_z, 2, n_tp)), dma((n_z, 2, n_tp)),
        dma((n_z, 2)), dma((n_z, 2)),
        dma((n_z,)), dma((n_z,)),
        dma((n_z,)), dma((n_z,)),
    ]
    return pl.pallas_call(
        functools.partial(kernel, n_sp, n_tp, cap),
        out_shape=jax.ShapeDtypeStruct((feats, pos), BF16),
        in_specs=[anywhere] * 17,
        out_specs=vmem,
        scratch_shapes=scratch,
        compiler_params=pltpu.CompilerParams(
            collective_id=0, has_side_effects=True, vmem_limit_bytes=64 * 1024 * 1024 - 65536
        ),
    )(
        stream, values_in, in_gate, out_gate, documents.reshape(1, pos), conv_taps,
        head_gain.reshape(1, chans), mix_weight, norm_gain.reshape(1, feats), routes.T,
        route_weight.T, expert_gate, expert_up, expert_down, shared_gate, shared_up, shared_down,
    )


def solution(mesh):
    in_specs = (
        P("tp", "sp"),
        P("tp", "sp"),
        P("tp", "sp"),
        P("tp", "sp"),
        P("sp"),
        P(None, "tp"),
        P("tp"),
        P("tp", None),
        P("tp"),
        P("sp", None),
        P("sp", None),
        P("sp", None, "tp"),
        P("sp", None, "tp"),
        P("sp", None, "tp"),
        P(None, "tp"),
        P(None, "tp"),
        P("tp", None),
    )
    body = functools.partial(local, mesh.shape["sp"], mesh.shape["tp"])
    return jax.shard_map(
        body, mesh=mesh, in_specs=in_specs, out_specs=P("tp", "sp"), check_vma=False
    )
```

```python
import functools

import jax
import jax.numpy as jnp
from jax import lax
from jax.experimental import pallas as pl
from jax.experimental.pallas import tpu as pltpu
from jax.sharding import PartitionSpec as P

HEAD = 64
CORES = 2
SUB = 8
EDGE = 16
epsilon = 1e-06
MESH = pl.DeviceIdType.MESH
F32 = jnp.float32
BF16 = jnp.bfloat16


def flipped(index, mask):
    bit = 1
    out = index
    while bit <= mask:
        if mask & bit:
            out = out + bit - 2 * bit * lax.rem(lax.div(index, bit), 2)
        bit *= 2
    return out


def dot(left, right):
    return jnp.dot(left, right, preferred_element_type=F32)


def silu(value):
    return value / (1.0 + jnp.exp(-value))


def column_of(row, width):
    return jnp.broadcast_to(row, (width, row.shape[1])).T


def kernel(
    n_sp, n_tp, cap,
    stream_h, values_h, in_h, out_h, documents_h, taps_h, head_h, mix_weight,
    norm_h, routes_h, route_weight_h, expert_gate, expert_up, expert_down,
    shared_gate, shared_up, shared_down,
    out,
    stream, values_in, in_gate, out_gate, documents, conv_taps, head_gain,
    norm_gain, routes, route_weight, mix_w, gate_w, up_w, sgate_w, sup_w, sdown_w, down_w,
    tail_s, prev_r, prev_docs, mix_s, mix_r, hidden_v, x_all, ss_s, ss_r, meta_r,
    sh_s, sh_r, mid_all, part_v, acc_v, pr_s, pr_r, zr_s, zr_r,
    small_sem, load_sem, halo_send, halo_recv, mix_send, mix_recv, ss_send, ss_recv,
    meta_send, meta_recv, xm_recv, xo_recv, xs_send, xb_send, sh_send, sh_recv,
    mid_send, mid_recv, fwd_recv, pr_recv, zr_recv,
):
    sp = lax.axis_index("sp")
    tp = lax.axis_index("tp")
    z = lax.div(sp, CORES)
    core = lax.rem(sp, CORES)
    n_z = n_sp // CORES
    feats, pos = stream.shape
    chans = values_in.shape[0]
    width = feats * n_tp
    hid = gate_w.shape[1]
    partner = {"sp": z * CORES + 1 - core}
    peers = [flipped(tp, d) for d in range(1, n_tp)]
    square = n_tp == 4 and n_z == 4
    near = peers[:2] if square else peers
    layers = [flipped(z, d) for d in range(n_z)]
    inner = lax.div(z + 1, 2) == 1
    if square:
        layers[2:] = [jnp.where(inner, layers[3], layers[2]), jnp.where(inner, layers[2], layers[3])]
    branch = [""]
    counts = {}

    def only(where, stage, *args):
        @pl.when(inner if where == "inner" else jnp.logical_not(inner))
        def _():
            branch[0] = where
            stage(*args)
            branch[0] = ""

    def far_own():
        for d in (2, 3):
            send(x_all.at[sp, tp], x_all.at[sp, tp], "x", xm_recv.at[z, tp],
                 {"sp": layers[d] * CORES + core})

    def onward(d, slice_of):
        block = x_all.at[layers[d] * CORES + core, slice_of]
        send(block, block, "x", xm_recv.at[layers[d], slice_of],
             {"sp": layers[2 if d < 2 else 1] * CORES + core})

    def across(d, slice_of):
        block = x_all.at[layers[d] * CORES + core, slice_of]
        send(block, block, "x", xo_recv.at[layers[d]], partner)

    def send(src, dst, kind, rsem, device):
        if isinstance(kind, str):
            key = (branch[0], kind)
            at = counts.get(key, 0)
            counts[key] = at + 1
            if kind == "mid":
                sem = mid_send.at[at // (2 * n_tp)]
            else:
                sem = (xb_send if branch[0] else xs_send).at[at // n_tp]
        else:
            sem = kind
        pltpu.make_async_remote_copy(
            src_ref=src, dst_ref=dst, send_sem=sem, recv_sem=rsem,
            device_id=device, device_id_type=MESH,
        ).start()

    def sent(like, sem):
        pltpu.make_async_remote_copy(
            src_ref=like, dst_ref=like, send_sem=sem, recv_sem=sem,
            device_id=partner, device_id_type=MESH,
        ).wait_send()

    def all_sent(where):
        for kind, size in (("x", n_tp), ("mid", 2 * n_tp)):
            left, at = counts.get((where, kind), 0), 0
            while left > 0:
                now = min(left, size)
                if kind == "x":
                    sent(x_all.at[0, pl.ds(0, now)], (xb_send if where else xs_send).at[at])
                else:
                    sent(mid_all.at[0, pl.ds(0, now // 2)], mid_send.at[at])
                left, at = left - now, at + 1

    def arrived(dst, rsem):
        pltpu.make_async_remote_copy(
            src_ref=dst, dst_ref=dst, send_sem=rsem, recv_sem=rsem,
            device_id=partner, device_id_type=MESH,
        ).wait_recv()

    loads = [
        pltpu.make_async_copy(src, dst, load_sem.at[i])
        for i, (src, dst) in enumerate([
            (mix_weight, mix_w), (shared_gate, sgate_w), (shared_up, sup_w),
            (shared_down, sdown_w), (expert_gate.at[0], gate_w), (expert_up.at[0], up_w),
            (expert_down.at[0], down_w),
        ])
    ]
    smalls = [
        pltpu.make_async_copy(src, dst, small_sem.at[i])
        for i, (src, dst) in enumerate([
            (values_h, values_in), (in_h, in_gate), (documents_h, documents), (out_h, out_gate),
            (taps_h, conv_taps), (head_h, head_gain), (routes_h, routes),
            (route_weight_h, route_weight), (stream_h, stream), (norm_h, norm_gain),
        ])
    ]

    barrier = pltpu.get_barrier_semaphore()
    for peer in peers:
        pl.semaphore_signal(barrier, inc=1, device_id={"tp": peer}, device_id_type=MESH)
    for d in range(1, n_sp):
        pl.semaphore_signal(
            barrier, inc=1, device_id={"sp": lax.rem(sp + d, n_sp)}, device_id_type=MESH
        )
    for copy in smalls:
        copy.start()
    loads[0].start()
    for copy in smalls[:3]:
        copy.wait()
    product = values_in[...].astype(F32) * in_gate[...].astype(F32)
    tail_s[...] = product.T[pos - SUB:, :]
    for copy in smalls[3:]:
        copy.wait()

    tap_rows = jnp.concatenate([conv_taps[...], jnp.zeros((SUB - 3, chans), F32)], axis=0).T
    taps = [jnp.broadcast_to(tap_rows[:, j:j + 1], (chans, pos)) for j in range(3)]
    docs = documents[...]
    lane_c = lax.broadcasted_iota(jnp.int32, (chans, pos), 1)
    lane_1 = lax.broadcasted_iota(jnp.int32, (1, pos), 1)

    def heads_of(before, docs_before):
        convolved = taps[2] * product
        for shift in (1, 2):
            moved = pltpu.roll(product, shift, 1)
            if before is not None:
                moved = jnp.where(lane_c < shift, pltpu.roll(before, shift, 1), moved)
            ids = jnp.where(lane_1 < shift, pltpu.roll(docs_before, shift, 1), pltpu.roll(docs, shift, 1))
            convolved = convolved + jnp.where(ids == docs, taps[2 - shift] * moved, 0.0)
        mixed = out_gate[...].astype(F32) * convolved
        heads = mixed.reshape(chans // HEAD, HEAD, pos)
        heads = heads * lax.rsqrt(jnp.mean(heads * heads, axis=1, keepdims=True) + epsilon)
        return (heads.reshape(chans, pos).T * head_gain[...]).astype(BF16)

    def mix(rows, heads_t):
        for b, peer in enumerate(peers + [tp]):
            cols = pl.ds(pl.multiple_of(peer * feats, feats), feats)
            mix_s[b, rows[0]:rows[1]] = dot(heads_t[rows[0]:rows[1]], mix_w[:, cols]).astype(BF16)

    def send_mix(rows):
        part = pl.ds(rows[0], rows[1] - rows[0])
        for b, peer in enumerate(peers):
            send(mix_s.at[b, part], mix_r.at[b, part], mix_send, mix_recv.at[b], {"tp": peer})

    heads_t = heads_of(None, jnp.full((1, pos), -1, jnp.int32))
    loads[0].wait()
    for load in loads[1:]:
        load.start()
    mix((EDGE, pos), heads_t)
    with jax.named_scope("barrier"):
        pl.semaphore_wait(barrier, n_tp - 1 + n_sp - 1)
    after = {"sp": lax.rem(sp + 1, n_sp)}
    halo = [
        pltpu.make_async_remote_copy(
            src_ref=src, dst_ref=dst, send_sem=halo_send.at[i], recv_sem=halo_recv.at[i],
            device_id=after, device_id_type=MESH,
        )
        for i, (src, dst) in enumerate([
            (tail_s, prev_r.at[pl.ds(pos - SUB, SUB)]), (documents, prev_docs),
        ])
    ]

    @pl.when(sp < n_sp - 1)
    def _():
        for copy in halo:
            copy.start()

    send_mix((EDGE, pos))

    @pl.when(sp == 0)
    def _():
        prev_r[...] = jnp.zeros((pos, chans), F32)
        prev_docs[...] = jnp.full((1, pos), -1, jnp.int32)

    @pl.when(sp > 0)
    def _():
        prev_r[: pos - SUB, :] = jnp.zeros((pos - SUB, chans), F32)
        with jax.named_scope("w_halo"):
            for copy in halo:
                copy.wait_recv()

    heads_t = heads_of(prev_r[...].T, prev_docs[...])
    mix((0, EDGE), heads_t)
    send_mix((0, EDGE))

    named = routes[...]
    weights = route_weight[...]
    meta_rows = meta_r.shape[1]
    at_row = lax.broadcasted_iota(jnp.int32, (meta_rows, pos), 0)
    table = jnp.zeros((meta_rows, pos), F32)
    for k in range(routes.shape[0]):
        table = table + jnp.where(at_row == named[k:k + 1, :], weights[k:k + 1, :], 0.0)
    stream_t = stream[...].astype(F32).T

    hidden = stream_t + mix_s[n_tp - 1].astype(F32)
    for b in range(n_tp - 1):
        with jax.named_scope(f"w_mix{b}"):
            arrived(mix_r.at[b], mix_recv.at[b])
        hidden = hidden + mix_r[b].astype(F32)
    hidden_v[...] = hidden
    x_all[sp, tp] = (hidden * norm_gain[...]).astype(BF16)
    squares = jnp.sum(hidden * hidden, axis=1, keepdims=True)
    row = jnp.broadcast_to(squares, (pos, pos)).T[:SUB]
    ss_s[...] = row
    for b, peer in enumerate(peers):
        send(ss_s, ss_r.at[b], ss_send, ss_recv, {"tp": peer})
    own = x_all.at[sp, tp]
    for b, peer in enumerate(peers):
        send(own, own, "x", xm_recv.at[z, tp], {"tp": peer})
    for d in ([1] if square else range(1, n_z)):
        send(own, own, "x", xm_recv.at[z, tp], {"sp": layers[d] * CORES + core})
    if square:
        only("inner", far_own)
    across(0, tp)

    with jax.named_scope("w_ss"):
        arrived(ss_r, ss_recv)
    for b in range(n_tp - 1):
        row = row + ss_r[b]
    scale = lax.rsqrt(row[:1] / width + epsilon)
    meta_r[sp] = jnp.where(at_row == meta_rows - 1, scale, table)
    for d in range(1, n_sp):
        send(meta_r.at[sp], meta_r.at[sp], meta_send, meta_recv.at[sp],
             {"sp": lax.rem(sp + d, n_sp)})

    def fetch(d, b):
        with jax.named_scope(f"w_x{d}_{b}"):
            arrived(x_all.at[layers[d] * CORES + core, peers[b]], xm_recv.at[layers[d], peers[b]])
        across(d, peers[b])

    def fetch_inner(d, b):
        fetch(d, b)
        onward(d, peers[b])

    def from_layer(d):
        block = x_all.at[layers[d] * CORES + core, tp]
        with jax.named_scope(f"w_layer{d}"):
            arrived(block, xm_recv.at[layers[d], tp])
        for b, peer in enumerate([] if square and d != 2 else near):
            send(block, block, "x", xm_recv.at[layers[d], tp], {"tp": peer})
        across(d, tp)

    def from_layer_inner(d):
        from_layer(d)
        if d != 2:
            onward(d, tp)

    def closer(b):
        block = x_all.at[sp, peers[b]]
        send(block, block, "x", xm_recv.at[z, peers[b]], {"sp": layers[1] * CORES + core})

    if square:
        only("inner", from_layer_inner, 1)
        only("inner", from_layer_inner, 2)

    with jax.named_scope("w_load"):
        for i in (1, 2, 3):
            loads[i].wait()
    scale_own = column_of(scale, pos)[:, :1]

    def shared_part(peer):
        rows = pl.ds(pl.multiple_of(peer * feats, feats), feats)
        block = x_all[sp, peer]
        return dot(block, sgate_w[rows, :]), dot(block, sup_w[rows, :])

    gate, upward = shared_part(tp)
    for b in range(n_tp - 1):
        fetch(0, b)
        if square:
            closer(b)
        if square and b == 2:
            only("inner", onward, 0, peers[2])
        more = shared_part(peers[b])
        gate, upward = gate + more[0], upward + more[1]
    shared_mid = (silu(gate * scale_own) * (upward * scale_own)).astype(BF16)
    half = pos // 2

    def shared_to(b, part, slot, i):
        part = pl.ds(part * half, half)
        rsem = sh_recv.at[1 + i] if slot == 2 else sh_recv.at[0]
        send(sh_s.at[b, part], sh_r.at[slot, part], sh_send, rsem, {"tp": peers[i]})

    for b in ([2, 0, 1, 3] if square else range(n_tp)):
        peer = (peers + [tp])[b]
        cols = pl.ds(pl.multiple_of(peer * feats, feats), feats)
        sh_s[b] = dot(shared_mid, sdown_w[:, cols]).astype(BF16)
        if square and b == 2:
            shared_to(2, 0, 2, 0)
            shared_to(2, 1, 2, 1)
        elif square and b < 2:
            shared_to(b, b, 0, b)
        elif b < n_tp - 1:
            send(sh_s.at[b], sh_r.at[b], sh_send, sh_recv.at[0], {"tp": peer})

    def shared_on(i):
        rows = slice(i * half, (i + 1) * half)
        with jax.named_scope(f"w_shared{i}"):
            arrived(sh_r.at[2, pl.ds(i * half, half)], sh_recv.at[1 + i])
        sh_s[1 - i, rows] = (sh_s[1 - i, rows].astype(F32) + sh_r[2, rows].astype(F32)).astype(BF16)
        shared_to(1 - i, i, 1, 1 - i)

    with jax.named_scope("w_load2"):
        for i in (4, 5, 6):
            loads[i].wait()

    at_a = lax.broadcasted_iota(jnp.int32, (pos, pos), 0)
    at_b = lax.broadcasted_iota(jnp.int32, (pos, pos), 1)
    earlier = jnp.where(at_a < at_b, 1.0, 0.0).astype(BF16)
    rank_row = lax.broadcasted_iota(jnp.int32, (cap, pos), 0).astype(F32)
    rank_lane = lax.broadcasted_iota(jnp.int32, (pos, cap), 1).astype(F32)

    def groups_of(d):
        return layers[d] * CORES + core, layers[d] * CORES + 1 - core

    def slots_of(group):
        weight = meta_r[group, pl.ds(sp, 1), :]
        mask = jnp.where(weight > 0.0, 1.0, 0.0)
        count = dot(jnp.broadcast_to(mask, (2 * SUB, pos)).astype(BF16), earlier)[:1]
        return weight, jnp.where(weight > 0.0, count, -1.0)

    def widen(d, which=(0, 1)):
        groups = [groups_of(d)[i] for i in which]
        for i, group in zip(which, groups):
            with jax.named_scope(f"w_group{d}_{i}"):
                if d > 0 or i > 0:
                    arrived(meta_r.at[group], meta_recv.at[group])
                if i > 0:
                    arrived(x_all.at[group], xo_recv.at[layers[d]])
        rows = len(groups) * pos
        gate = jnp.zeros((rows, hid), F32)
        upward = jnp.zeros((rows, hid), F32)
        for b in range(n_tp):
            block = jnp.concatenate([x_all[group, b] for group in groups], axis=0)
            gate = gate + dot(block, gate_w[b * feats:(b + 1) * feats, :])
            upward = upward + dot(block, up_w[b * feats:(b + 1) * feats, :])
        scales = jnp.concatenate([
            column_of(meta_r[group, meta_rows - 1:, :], pos)[:, :1] for group in groups
        ], axis=0)
        middle = (silu(gate * scales) * (upward * scales)).astype(BF16)
        for at, (i, group) in enumerate(zip(which, groups)):
            slot = slots_of(group)[1]
            pick = jnp.where(rank_row == slot, 1.0, 0.0).astype(BF16)
            mid_all[d, tp, i * cap:(i + 1) * cap, :] = dot(
                pick, middle[at * pos:(at + 1) * pos]
            ).astype(BF16)

    def mids(d, i):
        block = mid_all.at[d, tp, pl.ds(i * cap, cap)]
        for b, peer in enumerate(near):
            send(block, block, "mid", mid_recv.at[d, i, b], {"tp": peer})

    def relay(d, i):
        for b, peer in enumerate(near):
            part = mid_all.at[d, peer, pl.ds(i * cap, cap)]
            with jax.named_scope(f"w_mid{d}_{i}_{b}"):
                arrived(part, mid_recv.at[d, i, b])
            if square and b == i:
                send(part, part, "mid", fwd_recv.at[d], {"tp": near[1 - b]})

    def down(d, peer):
        rows = pl.ds(pl.multiple_of(peer * hid, hid), hid)
        return dot(mid_all[d, peer], down_w[rows, :])

    def gather(d):
        total = down(d, tp)
        for peer in near:
            total = total + down(d, peer)
        part_v[d] = total

    def narrow(d):
        if square:
            with jax.named_scope(f"w_fwd{d}"):
                arrived(mid_all.at[d, peers[2]], fwd_recv.at[d])
        total = part_v[d]
        if square:
            total = total + down(d, peers[2])
        total = total.astype(BF16)
        terms = []
        for i, group in enumerate(groups_of(d)):
            weight, slot = slots_of(group)
            place = jnp.where(rank_lane == column_of(slot, cap), 1.0, 0.0).astype(BF16)
            term = dot(place, total[i * cap:(i + 1) * cap])
            terms.append(term * column_of(weight, pos)[:, :1])
        acc_v[d] = terms[0]
        pr_s[d] = terms[1].astype(BF16)
        send(pr_s.at[d], pr_r.at[d], "x", pr_recv.at[d], partner)

    def join(d):
        with jax.named_scope(f"w_pr{d}"):
            arrived(pr_r.at[d], pr_recv.at[d])
        if d == 0:
            return
        total = acc_v[d] + pr_r[d].astype(F32)
        zr_s[d] = total.astype(BF16)
        slot = {"inner": (0, 1, 1), "end": (0, 2, 2)}[branch[0]][d - 1] if square else d - 1
        send(zr_s.at[d], zr_r.at[slot], "x", zr_recv, {"sp": layers[d] * CORES + core})

    def finish():
        result = hidden_v[...] + sh_s[n_tp - 1].astype(F32)
        blocks = 2 if square else n_tp - 1
        with jax.named_scope("w_sh"):
            arrived(sh_r.at[pl.ds(0, blocks)], sh_recv.at[0])
        for b in range(blocks):
            result = result + sh_r[b].astype(F32)
        result = result + acc_v[0] + pr_r[0].astype(F32)
        if n_z > 1:
            with jax.named_scope("w_zr"):
                arrived(zr_r, zr_recv)
        for d in range(1, n_z):
            result = result + zr_r[d - 1].astype(F32)
        out[...] = result.T.astype(BF16)
        with jax.named_scope("w_sent"):
            all_sent(branch[0])

    def run(plan):
        for stage, *where in plan:
            stage(*where)

    if square:
        plan = [(from_layer, 1), (widen, 0), (mids, 0, 0), (from_layer, 2), (mids, 0, 1)]
        plan += [(fetch, 1, b) for b in range(3)] + [(shared_on, 0), (shared_on, 1)]
        plan += [(widen, 1), (mids, 1, 0), (mids, 1, 1), (relay, 0, 0), (relay, 0, 1), (from_layer, 3)]
        plan += [(fetch, 2, b) for b in range(3)] + [(widen, 2), (mids, 2, 0), (mids, 2, 1)]
        plan += [(relay, 1, 0), (relay, 1, 1)] + [(fetch, 3, b) for b in range(3)]
        plan += [(widen, 3, (0,)), (mids, 3, 0), (widen, 3, (1,)), (mids, 3, 1)]
        plan += [(relay, 2, 0), (relay, 2, 1), (gather, 1), (narrow, 1), (gather, 2), (relay, 3, 0), (join, 1)]
        plan += [(gather, 0), (relay, 3, 1), (narrow, 2), (gather, 3), (join, 2), (narrow, 3)]
        plan += [(narrow, 0), (join, 3), (join, 0), (finish,)]
        only("end", run, plan)
        plan = [(from_layer_inner, 3), (widen, 0), (mids, 0, 0), (fetch_inner, 2, 2)]
        plan += [(fetch_inner, 1, b) for b in range(3)] + [(fetch, 2, 0), (fetch, 2, 1)]
        plan += [(shared_on, 0), (shared_on, 1), (widen, 1), (mids, 1, 0)]
        plan += [(widen, 2), (mids, 2, 0), (mids, 2, 1), (mids, 1, 1)]
        plan += [(fetch_inner, 3, b) for b in range(3)] + [(widen, 3), (mids, 3, 0), (mids, 3, 1)]
        plan += [(relay, 2, 0), (relay, 2, 1), (gather, 2), (relay, 3, 0), (relay, 3, 1)]
        plan += [(relay, 1, 0), (relay, 1, 1), (mids, 0, 1), (relay, 0, 0), (narrow, 2), (gather, 3)]
        plan += [(narrow, 3), (join, 2), (gather, 1), (join, 3), (narrow, 1), (join, 1)]
        plan += [(relay, 0, 1), (gather, 0), (narrow, 0), (join, 0), (finish,)]
        only("inner", run, plan)
    else:
        plan = [(from_layer, d) for d in range(1, n_z)]
        for d in range(n_z):
            plan += [(fetch, d, b) for b in range(n_tp - 1)] if d else []
            plan += [(widen, d), (mids, d, 0), (mids, d, 1)]
        for d in range(n_z):
            plan += [(relay, d, 0), (relay, d, 1), (gather, d), (narrow, d), (join, d)]
        run(plan + [(finish,)])

    with jax.named_scope("w_send"):
        all_sent("")
        sent(mix_s.at[pl.ds(0, n_tp - 1)], mix_send)
        sent(ss_r, ss_send)
        sent(meta_r.at[pl.ds(0, n_sp - 1)], meta_send)
        sent(sh_s.at[pl.ds(0, 3 if square else n_tp - 1)], sh_send)

        @pl.when(sp < n_sp - 1)
        def _():
            for copy in halo:
                copy.wait_send()


def local(n_sp, n_tp, *args):
    (stream, values_in, in_gate, out_gate, documents, conv_taps, head_gain, mix_weight,
     norm_gain, routes, route_weight, expert_gate, expert_up, expert_down,
     shared_gate, shared_up, shared_down) = args
    feats, pos = stream.shape
    chans = values_in.shape[0]
    width = feats * n_tp
    hid = expert_gate.shape[2]
    n_z = n_sp // CORES
    meta_rows = -(-(n_sp + 1) // SUB) * SUB
    experts = n_sp * expert_gate.shape[0]
    bound = 3 * pos * routes.shape[1] // (2 * experts)
    cap = -(-bound // (2 * SUB)) * 2 * SUB
    square = n_tp == 4 and n_z == 4
    near = 2 if square else n_tp - 1
    sends = (11, 34) if square else (n_tp * (2 * n_z + 1) * 2, 1)
    vmem = pl.BlockSpec(memory_space=pltpu.VMEM)
    anywhere = pl.BlockSpec(memory_space=pl.ANY)
    dma = pltpu.SemaphoreType.DMA
    scratch = [
        pltpu.VMEM((feats, pos), BF16),
        pltpu.VMEM((chans, pos), BF16),
        pltpu.VMEM((chans, pos), BF16),
        pltpu.VMEM((chans, pos), BF16),
        pltpu.VMEM((1, pos), jnp.int32),
        pltpu.VMEM(conv_taps.shape, F32),
        pltpu.VMEM((1, chans), F32),
        pltpu.VMEM((1, feats), F32),
        pltpu.VMEM((routes.shape[1], pos), jnp.int32),
        pltpu.VMEM((routes.shape[1], pos), F32),
        pltpu.VMEM((chans, width), BF16),
        pltpu.VMEM((width, hid), BF16),
        pltpu.VMEM((width, hid), BF16),
        pltpu.VMEM((width, hid), BF16),
        pltpu.VMEM((width, hid), BF16),
        pltpu.VMEM((hid, width), BF16),
        pltpu.VMEM((n_tp * hid, feats), BF16),
        pltpu.VMEM((SUB, chans), F32),
        pltpu.VMEM((pos, chans), F32),
        pltpu.VMEM((1, pos), jnp.int32),
        pltpu.VMEM((n_tp, pos, feats), BF16),
        pltpu.VMEM((n_tp, pos, feats), BF16),
        pltpu.VMEM((pos, feats), F32),
        pltpu.VMEM((n_sp, n_tp, pos, feats), BF16),
        pltpu.VMEM((SUB, pos), F32),
        pltpu.VMEM((n_tp - 1, SUB, pos), F32),
        pltpu.VMEM((n_sp, meta_rows, pos), F32),
        pltpu.VMEM((n_tp, pos, feats), BF16),
        pltpu.VMEM((n_tp, pos, feats), BF16),
        pltpu.VMEM((n_z, n_tp, CORES * cap, hid), BF16),
        pltpu.VMEM((n_z, CORES * cap, feats), F32),
        pltpu.VMEM((n_z, pos, feats), F32),
        pltpu.VMEM((n_z, pos, feats), BF16),
        pltpu.VMEM((n_z, pos, feats), BF16),
        pltpu.VMEM((n_z, pos, feats), BF16),
        pltpu.VMEM((max(n_z - 1, 1), pos, feats), BF16),
        dma((10,)), dma((7,)),
        dma((2,)), dma((2,)),
        dma, dma((n_tp - 1,)),
        dma, dma,
        dma, dma((n_sp,)),
        dma((n_z, n_tp)), dma((n_z,)), dma((-(-sends[0] // n_tp),)), dma((-(-sends[1] // n_tp),)),
        dma, dma((3,)),
        dma((n_z,)), dma((n_z, 2, near)), dma((n_z,)),
        dma((n_z,)), dma,
    ]
    return pl.pallas_call(
        functools.partial(kernel, n_sp, n_tp, cap),
        out_shape=pltpu.VMEM((feats, pos), BF16),
        in_specs=[anywhere] * 17,
        out_specs=vmem,
        scratch_shapes=scratch,
        compiler_params=pltpu.CompilerParams(
            collective_id=0, has_side_effects=True,
            vmem_limit_bytes=64 * 1024 * 1024 - 65536 - 2 * feats * pos,
        ),
    )(
        stream, values_in, in_gate, out_gate, documents.reshape(1, pos), conv_taps,
        head_gain.reshape(1, chans), mix_weight, norm_gain.reshape(1, feats), routes.T,
        route_weight.T, expert_gate, expert_up, expert_down, shared_gate, shared_up, shared_down,
    )


def solution(mesh):
    in_specs = (
        P("tp", "sp"),
        P("tp", "sp"),
        P("tp", "sp"),
        P("tp", "sp"),
        P("sp"),
        P(None, "tp"),
        P("tp"),
        P("tp", None),
        P("tp"),
        P("sp", None),
        P("sp", None),
        P("sp", None, "tp"),
        P("sp", None, "tp"),
        P("sp", None, "tp"),
        P(None, "tp"),
        P(None, "tp"),
        P("tp", None),
    )
    body = functools.partial(local, mesh.shape["sp"], mesh.shape["tp"])
    return jax.shard_map(
        body, mesh=mesh, in_specs=in_specs, out_specs=P("tp", "sp"), check_vma=False
    )
```

```python
import functools

import jax
import jax.numpy as jnp
from jax import lax
from jax.experimental import pallas as pl
from jax.experimental.pallas import tpu as pltpu
from jax.sharding import PartitionSpec as P

HEAD = 64
CORES = 2
SUB = 8
EDGE = 16
epsilon = 1e-06
MESH = pl.DeviceIdType.MESH
F32 = jnp.float32
BF16 = jnp.bfloat16


def flipped(index, mask):
    bit = 1
    out = index
    while bit <= mask:
        if mask & bit:
            out = out + bit - 2 * bit * lax.rem(lax.div(index, bit), 2)
        bit *= 2
    return out


def dot(left, right):
    return jnp.dot(left, right, preferred_element_type=F32)


def silu(value):
    return value / (1.0 + jnp.exp(-value))


def column_of(row, width):
    return jnp.broadcast_to(row, (width, row.shape[1])).T


def kernel(
    n_sp, n_tp, cap,
    stream_h, values_h, in_h, out_h, documents_h, taps_h, head_h, mix_weight,
    norm_h, routes_h, route_weight_h, expert_gate, expert_up, expert_down,
    shared_gate, shared_up, shared_down,
    out,
    stream, values_in, in_gate, out_gate, documents, conv_taps, head_gain,
    norm_gain, routes, route_weight, mix_w, gate_w, up_w, sgate_w, sup_w, sdown_w, down_w,
    tail_s, prev_r, prev_docs, mix_s, mix_r, hidden_v, x_all, ss_s, ss_r, meta_r,
    sh_s, sh_r, mid_all, part_v, place_v, column_v, early_v, acc_v, pr_s, pr_r, zr_s, zr_r,
    small_sem, load_sem, halo_send, halo_recv, mix_send, mix_recv, ss_send, ss_recv,
    meta_send, meta_recv, xm_recv, xo_recv, xs_send, xb_send, sh_send, sh_recv,
    mid_send, mid_recv, fwd_recv, pr_recv, zr_recv,
):
    sp = lax.axis_index("sp")
    tp = lax.axis_index("tp")
    z = lax.div(sp, CORES)
    core = lax.rem(sp, CORES)
    n_z = n_sp // CORES
    feats, pos = stream.shape
    chans = values_in.shape[0]
    width = feats * n_tp
    hid = gate_w.shape[1]
    partner = {"sp": z * CORES + 1 - core}
    peers = [flipped(tp, d) for d in range(1, n_tp)]
    square = n_tp == 4 and n_z == 4
    near = peers[:2] if square else peers
    layers = [flipped(z, d) for d in range(n_z)]
    inner = lax.div(z + 1, 2) == 1
    if square:
        layers[2:] = [jnp.where(inner, layers[3], layers[2]), jnp.where(inner, layers[2], layers[3])]
    branch = [""]
    counts = {}

    def only(where, stage, *args):
        @pl.when(inner if where == "inner" else jnp.logical_not(inner))
        def _():
            branch[0] = where
            stage(*args)
            branch[0] = ""

    def far_own():
        for d in (2, 3):
            send(x_all.at[sp, tp], x_all.at[sp, tp], "x", xm_recv.at[z, tp],
                 {"sp": layers[d] * CORES + core})

    def onward(d, slice_of):
        block = x_all.at[layers[d] * CORES + core, slice_of]
        send(block, block, "x", xm_recv.at[layers[d], slice_of],
             {"sp": layers[2 if d < 2 else 1] * CORES + core})

    def across(d, slice_of):
        block = x_all.at[layers[d] * CORES + core, slice_of]
        send(block, block, "x", xo_recv.at[layers[d]], partner)

    def send(src, dst, kind, rsem, device):
        if isinstance(kind, str):
            key = (branch[0], kind)
            at = counts.get(key, 0)
            counts[key] = at + 1
            if kind == "mid":
                sem = mid_send.at[at // (2 * n_tp)]
            else:
                sem = (xb_send if branch[0] else xs_send).at[at // n_tp]
        else:
            sem = kind
        pltpu.make_async_remote_copy(
            src_ref=src, dst_ref=dst, send_sem=sem, recv_sem=rsem,
            device_id=device, device_id_type=MESH,
        ).start()

    def sent(like, sem):
        pltpu.make_async_remote_copy(
            src_ref=like, dst_ref=like, send_sem=sem, recv_sem=sem,
            device_id=partner, device_id_type=MESH,
        ).wait_send()

    def all_sent(where):
        for kind, size in (("x", n_tp), ("mid", 2 * n_tp)):
            left, at = counts.get((where, kind), 0), 0
            while left > 0:
                now = min(left, size)
                if kind == "x":
                    sent(x_all.at[0, pl.ds(0, now)], (xb_send if where else xs_send).at[at])
                else:
                    sent(mid_all.at[0, pl.ds(0, now // 2)], mid_send.at[at])
                left, at = left - now, at + 1

    def arrived(dst, rsem):
        pltpu.make_async_remote_copy(
            src_ref=dst, dst_ref=dst, send_sem=rsem, recv_sem=rsem,
            device_id=partner, device_id_type=MESH,
        ).wait_recv()

    loads = [
        pltpu.make_async_copy(src, dst, load_sem.at[i])
        for i, (src, dst) in enumerate([
            (mix_weight, mix_w), (shared_gate, sgate_w), (shared_up, sup_w),
            (shared_down, sdown_w), (expert_gate.at[0], gate_w), (expert_up.at[0], up_w),
            (expert_down.at[0], down_w),
        ])
    ]
    smalls = [
        pltpu.make_async_copy(src, dst, small_sem.at[i])
        for i, (src, dst) in enumerate([
            (values_h, values_in), (in_h, in_gate), (documents_h, documents), (out_h, out_gate),
            (taps_h, conv_taps), (head_h, head_gain), (routes_h, routes),
            (route_weight_h, route_weight), (stream_h, stream), (norm_h, norm_gain),
        ])
    ]

    barrier = pltpu.get_barrier_semaphore()
    for peer in peers:
        pl.semaphore_signal(barrier, inc=1, device_id={"tp": peer}, device_id_type=MESH)
    for d in range(1, n_sp):
        pl.semaphore_signal(
            barrier, inc=1, device_id={"sp": lax.rem(sp + d, n_sp)}, device_id_type=MESH
        )
    for copy in smalls:
        copy.start()
    loads[0].start()
    for copy in smalls[:3]:
        copy.wait()
    product = values_in[...].astype(F32) * in_gate[...].astype(F32)
    tail_s[...] = product.T[pos - SUB:, :]
    for copy in smalls[3:]:
        copy.wait()

    tap_rows = jnp.concatenate([conv_taps[...], jnp.zeros((SUB - 3, chans), F32)], axis=0).T
    taps = [jnp.broadcast_to(tap_rows[:, j:j + 1], (chans, pos)) for j in range(3)]
    docs = documents[...]
    lane_c = lax.broadcasted_iota(jnp.int32, (chans, pos), 1)
    lane_1 = lax.broadcasted_iota(jnp.int32, (1, pos), 1)

    def heads_of(before, docs_before):
        convolved = taps[2] * product
        for shift in (1, 2):
            moved = pltpu.roll(product, shift, 1)
            if before is not None:
                moved = jnp.where(lane_c < shift, pltpu.roll(before, shift, 1), moved)
            ids = jnp.where(lane_1 < shift, pltpu.roll(docs_before, shift, 1), pltpu.roll(docs, shift, 1))
            convolved = convolved + jnp.where(ids == docs, taps[2 - shift] * moved, 0.0)
        mixed = out_gate[...].astype(F32) * convolved
        heads = mixed.reshape(chans // HEAD, HEAD, pos)
        heads = heads * lax.rsqrt(jnp.mean(heads * heads, axis=1, keepdims=True) + epsilon)
        return (heads.reshape(chans, pos).T * head_gain[...]).astype(BF16)

    def mix(rows, heads_t):
        for b, peer in enumerate(peers + [tp]):
            cols = pl.ds(pl.multiple_of(peer * feats, feats), feats)
            mix_s[b, rows[0]:rows[1]] = dot(heads_t[rows[0]:rows[1]], mix_w[:, cols]).astype(BF16)

    def mix_part(b, rows, slot, i, rsem):
        part = pl.ds(rows[0], rows[1] - rows[0])
        send(mix_s.at[b, part], mix_r.at[slot, part], mix_send, mix_recv.at[rsem], {"tp": peers[i]})

    parts = ((EDGE, pos // 2), (pos // 2, pos))

    def mix_on(i):
        rows = slice(*parts[i])
        with jax.named_scope(f"w_mixd{i}"):
            arrived(mix_r.at[2, pl.ds(parts[i][0], parts[i][1] - parts[i][0])], mix_recv.at[2 + i])
        mix_s[1 - i, rows] = (mix_s[1 - i, rows].astype(F32) + mix_r[2, rows].astype(F32)).astype(BF16)
        mix_part(1 - i, parts[i], 1, 1 - i, 1)

    def send_mix(rows):
        part = pl.ds(rows[0], rows[1] - rows[0])
        for b, peer in enumerate(peers):
            send(mix_s.at[b, part], mix_r.at[b, part], mix_send, mix_recv.at[b], {"tp": peer})

    heads_t = heads_of(None, jnp.full((1, pos), -1, jnp.int32))
    loads[0].wait()
    for load in loads[1:]:
        load.start()
    mix((EDGE, pos), heads_t)
    with jax.named_scope("barrier"):
        pl.semaphore_wait(barrier, n_tp - 1 + n_sp - 1)
    after = {"sp": lax.rem(sp + 1, n_sp)}
    halo = [
        pltpu.make_async_remote_copy(
            src_ref=src, dst_ref=dst, send_sem=halo_send.at[i], recv_sem=halo_recv.at[i],
            device_id=after, device_id_type=MESH,
        )
        for i, (src, dst) in enumerate([
            (tail_s, prev_r.at[pl.ds(pos - SUB, SUB)]), (documents, prev_docs),
        ])
    ]

    @pl.when(sp < n_sp - 1)
    def _():
        for copy in halo:
            copy.start()

    if square:
        for i in range(2):
            mix_part(2, parts[i], 2, i, 2 + i)
        for i in range(2):
            mix_part(i, parts[i], 0, i, 0)
    else:
        send_mix((EDGE, pos))

    @pl.when(sp == 0)
    def _():
        prev_r[...] = jnp.zeros((pos, chans), F32)
        prev_docs[...] = jnp.full((1, pos), -1, jnp.int32)

    @pl.when(sp > 0)
    def _():
        prev_r[: pos - SUB, :] = jnp.zeros((pos - SUB, chans), F32)
        with jax.named_scope("w_halo"):
            for copy in halo:
                copy.wait_recv()

    heads_t = heads_of(prev_r[...].T, prev_docs[...])
    mix((0, EDGE), heads_t)
    if square:
        for b in (2, 0, 1):
            mix_part(b, (0, EDGE), b, b, 4)
        mix_on(0)
        mix_on(1)
    else:
        send_mix((0, EDGE))

    named = routes[...]
    weights = route_weight[...]
    meta_rows = meta_r.shape[1]
    at_row = lax.broadcasted_iota(jnp.int32, (meta_rows, pos), 0)
    table = jnp.zeros((meta_rows, pos), F32)
    for k in range(routes.shape[0]):
        table = table + jnp.where(at_row == named[k:k + 1, :], weights[k:k + 1, :], 0.0)
    stream_t = stream[...].astype(F32).T

    hidden = stream_t + mix_s[n_tp - 1].astype(F32)
    if square:
        with jax.named_scope("w_mix"):
            arrived(mix_r.at[0, pl.ds(EDGE, pos - EDGE)], mix_recv.at[0])
            arrived(mix_r.at[1, pl.ds(EDGE, pos - EDGE)], mix_recv.at[1])
            arrived(mix_r.at[2, pl.ds(0, 3 * EDGE)], mix_recv.at[4])
        hidden = hidden + mix_r[0].astype(F32) + mix_r[1].astype(F32)
        edge = mix_r[2, :EDGE].astype(F32)
        hidden = hidden + jnp.concatenate([edge, jnp.zeros((pos - EDGE, feats), F32)], axis=0)
    for b in range(0 if square else n_tp - 1):
        with jax.named_scope(f"w_mix{b}"):
            arrived(mix_r.at[b], mix_recv.at[b])
        hidden = hidden + mix_r[b].astype(F32)
    hidden_v[...] = hidden
    x_all[sp, tp] = (hidden * norm_gain[...]).astype(BF16)
    squares = jnp.sum(hidden * hidden, axis=1, keepdims=True)
    row = jnp.broadcast_to(squares, (pos, pos)).T[:SUB]
    ss_s[...] = row
    for b, peer in enumerate(peers):
        send(ss_s, ss_r.at[b], ss_send, ss_recv, {"tp": peer})
    own = x_all.at[sp, tp]
    for b, peer in enumerate(peers):
        send(own, own, "x", xm_recv.at[z, tp], {"tp": peer})
    for d in ([1] if square else range(1, n_z)):
        send(own, own, "x", xm_recv.at[z, tp], {"sp": layers[d] * CORES + core})
    if square:
        only("inner", far_own)
    across(0, tp)

    with jax.named_scope("w_ss"):
        arrived(ss_r, ss_recv)
    for b in range(n_tp - 1):
        row = row + ss_r[b]
    scale = lax.rsqrt(row[:1] / width + epsilon)
    meta_r[sp] = jnp.where(at_row == meta_rows - 1, scale, table)
    for d in range(1, n_sp):
        send(meta_r.at[sp], meta_r.at[sp], meta_send, meta_recv.at[sp],
             {"sp": lax.rem(sp + d, n_sp)})

    def fetch(d, b):
        with jax.named_scope(f"w_x{d}_{b}"):
            arrived(x_all.at[layers[d] * CORES + core, peers[b]], xm_recv.at[layers[d], peers[b]])
        across(d, peers[b])

    def fetch_inner(d, b):
        fetch(d, b)
        onward(d, peers[b])

    def from_layer(d):
        block = x_all.at[layers[d] * CORES + core, tp]
        with jax.named_scope(f"w_layer{d}"):
            arrived(block, xm_recv.at[layers[d], tp])
        for b, peer in enumerate([] if square and d != 2 else near):
            send(block, block, "x", xm_recv.at[layers[d], tp], {"tp": peer})
        across(d, tp)

    def from_layer_inner(d):
        from_layer(d)
        if d != 2:
            onward(d, tp)

    def closer(b):
        block = x_all.at[sp, peers[b]]
        send(block, block, "x", xm_recv.at[z, peers[b]], {"sp": layers[1] * CORES + core})

    if square:
        only("inner", from_layer_inner, 1)
        only("inner", from_layer_inner, 2)

    with jax.named_scope("w_load"):
        for i in (1, 2, 3):
            loads[i].wait()
    scale_own = column_of(scale, pos)[:, :1]

    def shared_part(peer):
        rows = pl.ds(pl.multiple_of(peer * feats, feats), feats)
        block = x_all[sp, peer]
        return dot(block, sgate_w[rows, :]), dot(block, sup_w[rows, :])

    gate, upward = shared_part(tp)
    for b in range(n_tp - 1):
        fetch(0, b)
        if square:
            closer(b)
        if square and b == 2:
            only("inner", onward, 0, peers[2])
        more = shared_part(peers[b])
        gate, upward = gate + more[0], upward + more[1]
    shared_mid = (silu(gate * scale_own) * (upward * scale_own)).astype(BF16)
    half = pos // 2

    def shared_to(b, part, slot, i):
        part = pl.ds(part * half, half)
        rsem = sh_recv.at[1 + i] if slot == 2 else sh_recv.at[0]
        send(sh_s.at[b, part], sh_r.at[slot, part], sh_send, rsem, {"tp": peers[i]})

    for b in ([2, 0, 1, 3] if square else range(n_tp)):
        peer = (peers + [tp])[b]
        cols = pl.ds(pl.multiple_of(peer * feats, feats), feats)
        sh_s[b] = dot(shared_mid, sdown_w[:, cols]).astype(BF16)
        if square and b == 2:
            shared_to(2, 0, 2, 0)
            shared_to(2, 1, 2, 1)
        elif square and b < 2:
            shared_to(b, b, 0, b)
        elif b < n_tp - 1:
            send(sh_s.at[b], sh_r.at[b], sh_send, sh_recv.at[0], {"tp": peer})

    def shared_on(i):
        rows = slice(i * half, (i + 1) * half)
        with jax.named_scope(f"w_shared{i}"):
            arrived(sh_r.at[2, pl.ds(i * half, half)], sh_recv.at[1 + i])
        sh_s[1 - i, rows] = (sh_s[1 - i, rows].astype(F32) + sh_r[2, rows].astype(F32)).astype(BF16)
        shared_to(1 - i, i, 1, 1 - i)

    with jax.named_scope("w_load2"):
        for i in (4, 5, 6):
            loads[i].wait()

    at_a = lax.broadcasted_iota(jnp.int32, (pos, pos), 0)
    at_b = lax.broadcasted_iota(jnp.int32, (pos, pos), 1)
    earlier = jnp.where(at_a < at_b, 1.0, 0.0).astype(BF16)
    rank_row = lax.broadcasted_iota(jnp.int32, (cap, pos), 0).astype(F32)
    rank_lane = lax.broadcasted_iota(jnp.int32, (pos, cap), 1).astype(F32)

    def groups_of(d):
        return layers[d] * CORES + core, layers[d] * CORES + 1 - core

    def slots_of(group):
        weight = meta_r[group, pl.ds(sp, 1), :]
        mask = jnp.where(weight > 0.0, 1.0, 0.0)
        count = dot(jnp.broadcast_to(mask, (2 * SUB, pos)).astype(BF16), earlier)[:1]
        return weight, jnp.where(weight > 0.0, count, -1.0)

    def expert_part(group, peer):
        rows = pl.ds(pl.multiple_of(peer * feats, feats), feats)
        block = x_all[group, peer]
        return dot(block, gate_w[rows, :]), dot(block, up_w[rows, :])

    def begin(d):
        parts = [expert_part(groups_of(d)[0], peer) for peer in (tp, *near)]
        for i in range(2):
            early_v[i] = sum([part[i] for part in parts[1:]], parts[0][i])

    def widen(d, which=(0, 1), ready=False):
        groups = [groups_of(d)[i] for i in which]
        for i, group in zip(which, groups):
            with jax.named_scope(f"w_group{d}_{i}"):
                if d > 0 or i > 0:
                    arrived(meta_r.at[group], meta_recv.at[group])
                if i > 0:
                    arrived(x_all.at[group], xo_recv.at[layers[d]])
        rows = len(groups) * pos
        gate = jnp.zeros((rows, hid), F32)
        upward = jnp.zeros((rows, hid), F32)
        if ready:
            more = expert_part(groups[0], peers[2])
            gate, upward = early_v[0] + more[0], early_v[1] + more[1]
        for b in range(0 if ready else n_tp):
            block = jnp.concatenate([x_all[group, b] for group in groups], axis=0)
            gate = gate + dot(block, gate_w[b * feats:(b + 1) * feats, :])
            upward = upward + dot(block, up_w[b * feats:(b + 1) * feats, :])
        scales = jnp.concatenate([
            column_of(meta_r[group, meta_rows - 1:, :], pos)[:, :1] for group in groups
        ], axis=0)
        middle = (silu(gate * scales) * (upward * scales)).astype(BF16)
        for at, (i, group) in enumerate(zip(which, groups)):
            slot = slots_of(group)[1]
            pick = jnp.where(rank_row == slot, 1.0, 0.0).astype(BF16)
            mid_all[d, tp, i * cap:(i + 1) * cap, :] = dot(
                pick, middle[at * pos:(at + 1) * pos]
            ).astype(BF16)

    def mids(d, i):
        block = mid_all.at[d, tp, pl.ds(i * cap, cap)]
        for b, peer in enumerate(near):
            send(block, block, "mid", mid_recv.at[d, i, b], {"tp": peer})

    def relay(d, i):
        for b, peer in enumerate(near):
            part = mid_all.at[d, peer, pl.ds(i * cap, cap)]
            with jax.named_scope(f"w_mid{d}_{i}_{b}"):
                arrived(part, mid_recv.at[d, i, b])
            if square and b == i:
                send(part, part, "mid", fwd_recv.at[d], {"tp": near[1 - b]})

    def down(d, peer):
        rows = pl.ds(pl.multiple_of(peer * hid, hid), hid)
        return dot(mid_all[d, peer], down_w[rows, :])

    def gather(d):
        total = down(d, tp)
        for peer in near:
            total = total + down(d, peer)
        part_v[d] = total
        for i, group in enumerate(groups_of(d)):
            weight, slot = slots_of(group)
            place_v[d, i] = jnp.where(rank_lane == column_of(slot, cap), 1.0, 0.0).astype(BF16)
            column_v[d, i] = column_of(weight, pos)

    def narrow(d):
        if square:
            with jax.named_scope(f"w_fwd{d}"):
                arrived(mid_all.at[d, peers[2]], fwd_recv.at[d])
        total = part_v[d]
        if square:
            total = total + down(d, peers[2])
        total = total.astype(BF16)
        for i in (1, 0):
            term = dot(place_v[d, i], total[i * cap:(i + 1) * cap]) * column_v[d, i][:, :1]
            if i == 1:
                pr_s[d] = term.astype(BF16)
                send(pr_s.at[d], pr_r.at[d], "x", pr_recv.at[d], partner)
            else:
                acc_v[d] = term

    def join(d):
        with jax.named_scope(f"w_pr{d}"):
            arrived(pr_r.at[d], pr_recv.at[d])
        if d == 0:
            return
        total = acc_v[d] + pr_r[d].astype(F32)
        zr_s[d] = total.astype(BF16)
        slot = {"inner": (0, 1, 1), "end": (0, 2, 2)}[branch[0]][d - 1] if square else d - 1
        send(zr_s.at[d], zr_r.at[slot], "x", zr_recv, {"sp": layers[d] * CORES + core})

    def finish():
        result = hidden_v[...] + sh_s[n_tp - 1].astype(F32)
        blocks = 2 if square else n_tp - 1
        with jax.named_scope("w_sh"):
            arrived(sh_r.at[pl.ds(0, blocks)], sh_recv.at[0])
        for b in range(blocks):
            result = result + sh_r[b].astype(F32)
        result = result + acc_v[0] + pr_r[0].astype(F32)
        if n_z > 1:
            with jax.named_scope("w_zr"):
                arrived(zr_r, zr_recv)
        for d in range(1, n_z):
            result = result + zr_r[d - 1].astype(F32)
        out[...] = result.T.astype(BF16)
        with jax.named_scope("w_sent"):
            all_sent(branch[0])

    def run(plan):
        for stage, *where in plan:
            stage(*where)

    if square:
        plan = [(from_layer, 1), (widen, 0), (mids, 0, 0), (from_layer, 2), (mids, 0, 1)]
        plan += [(fetch, 1, b) for b in range(3)] + [(shared_on, 0), (shared_on, 1)]
        plan += [(widen, 1), (mids, 1, 0), (mids, 1, 1), (relay, 0, 0), (relay, 0, 1), (from_layer, 3)]
        plan += [(fetch, 2, b) for b in range(3)] + [(widen, 2), (mids, 2, 0), (mids, 2, 1)]
        plan += [(relay, 1, 0), (relay, 1, 1), (fetch, 3, 0), (fetch, 3, 1), (begin, 3), (fetch, 3, 2)]
        plan += [(widen, 3, (0,), True), (mids, 3, 0), (widen, 3, (1,)), (mids, 3, 1)]
        plan += [(relay, 2, 0), (relay, 2, 1), (gather, 1), (narrow, 1), (gather, 2), (relay, 3, 0), (join, 1)]
        plan += [(gather, 0), (relay, 3, 1), (narrow, 2), (gather, 3), (join, 2), (narrow, 3)]
        plan += [(narrow, 0), (join, 3), (join, 0), (finish,)]
        only("end", run, plan)
        plan = [(from_layer_inner, 3), (widen, 0), (mids, 0, 0), (fetch_inner, 2, 2)]
        plan += [(fetch_inner, 1, b) for b in range(3)] + [(fetch, 2, 0), (fetch, 2, 1)]
        plan += [(shared_on, 0), (shared_on, 1), (widen, 1), (mids, 1, 0)]
        plan += [(widen, 2), (mids, 2, 0), (mids, 2, 1), (mids, 1, 1)]
        plan += [(fetch_inner, 3, b) for b in range(3)] + [(widen, 3), (mids, 3, 0), (mids, 3, 1)]
        plan += [(relay, 2, 0), (relay, 2, 1), (gather, 2), (relay, 3, 0), (relay, 3, 1)]
        plan += [(relay, 1, 0), (relay, 1, 1), (mids, 0, 1), (relay, 0, 0), (narrow, 2), (gather, 3)]
        plan += [(narrow, 3), (join, 2), (gather, 1), (join, 3), (narrow, 1), (join, 1)]
        plan += [(relay, 0, 1), (gather, 0), (narrow, 0), (join, 0), (finish,)]
        only("inner", run, plan)
    else:
        plan = [(from_layer, d) for d in range(1, n_z)]
        for d in range(n_z):
            plan += [(fetch, d, b) for b in range(n_tp - 1)] if d else []
            plan += [(widen, d), (mids, d, 0), (mids, d, 1)]
        for d in range(n_z):
            plan += [(relay, d, 0), (relay, d, 1), (gather, d), (narrow, d), (join, d)]
        run(plan + [(finish,)])

    with jax.named_scope("w_send"):
        all_sent("")
        sent(mix_s.at[pl.ds(0, n_tp - 1)], mix_send)
        sent(ss_r, ss_send)
        sent(meta_r.at[pl.ds(0, n_sp - 1)], meta_send)
        sent(sh_s.at[pl.ds(0, 3 if square else n_tp - 1)], sh_send)

        @pl.when(sp < n_sp - 1)
        def _():
            for copy in halo:
                copy.wait_send()


def local(n_sp, n_tp, *args):
    (stream, values_in, in_gate, out_gate, documents, conv_taps, head_gain, mix_weight,
     norm_gain, routes, route_weight, expert_gate, expert_up, expert_down,
     shared_gate, shared_up, shared_down) = args
    feats, pos = stream.shape
    chans = values_in.shape[0]
    width = feats * n_tp
    hid = expert_gate.shape[2]
    n_z = n_sp // CORES
    meta_rows = -(-(n_sp + 1) // SUB) * SUB
    experts = n_sp * expert_gate.shape[0]
    bound = 3 * pos * routes.shape[1] // (2 * experts)
    cap = -(-bound // (2 * SUB)) * 2 * SUB
    square = n_tp == 4 and n_z == 4
    near = 2 if square else n_tp - 1
    sends = (11, 34) if square else (n_tp * (2 * n_z + 1) * 2, 1)
    vmem = pl.BlockSpec(memory_space=pltpu.VMEM)
    anywhere = pl.BlockSpec(memory_space=pl.ANY)
    dma = pltpu.SemaphoreType.DMA
    scratch = [
        pltpu.VMEM((feats, pos), BF16),
        pltpu.VMEM((chans, pos), BF16),
        pltpu.VMEM((chans, pos), BF16),
        pltpu.VMEM((chans, pos), BF16),
        pltpu.VMEM((1, pos), jnp.int32),
        pltpu.VMEM(conv_taps.shape, F32),
        pltpu.VMEM((1, chans), F32),
        pltpu.VMEM((1, feats), F32),
        pltpu.VMEM((routes.shape[1], pos), jnp.int32),
        pltpu.VMEM((routes.shape[1], pos), F32),
        pltpu.VMEM((chans, width), BF16),
        pltpu.VMEM((width, hid), BF16),
        pltpu.VMEM((width, hid), BF16),
        pltpu.VMEM((width, hid), BF16),
        pltpu.VMEM((width, hid), BF16),
        pltpu.VMEM((hid, width), BF16),
        pltpu.VMEM((n_tp * hid, feats), BF16),
        pltpu.VMEM((SUB, chans), F32),
        pltpu.VMEM((pos, chans), F32),
        pltpu.VMEM((1, pos), jnp.int32),
        pltpu.VMEM((n_tp, pos, feats), BF16),
        pltpu.VMEM((n_tp, pos, feats), BF16),
        pltpu.VMEM((pos, feats), F32),
        pltpu.VMEM((n_sp, n_tp, pos, feats), BF16),
        pltpu.VMEM((SUB, pos), F32),
        pltpu.VMEM((n_tp - 1, SUB, pos), F32),
        pltpu.VMEM((n_sp, meta_rows, pos), F32),
        pltpu.VMEM((n_tp, pos, feats), BF16),
        pltpu.VMEM((n_tp, pos, feats), BF16),
        pltpu.VMEM((n_z, n_tp, CORES * cap, hid), BF16),
        pltpu.VMEM((n_z, CORES * cap, feats), F32),
        pltpu.VMEM((n_z, CORES, pos, cap), BF16),
        pltpu.VMEM((n_z, CORES, pos, pos), F32),
        pltpu.VMEM((2, pos, hid), F32),
        pltpu.VMEM((n_z, pos, feats), F32),
        pltpu.VMEM((n_z, pos, feats), BF16),
        pltpu.VMEM((n_z, pos, feats), BF16),
        pltpu.VMEM((n_z, pos, feats), BF16),
        pltpu.VMEM((max(n_z - 1, 1), pos, feats), BF16),
        dma((10,)), dma((7,)),
        dma((2,)), dma((2,)),
        dma, dma((max(n_tp - 1, 5),)),
        dma, dma,
        dma, dma((n_sp,)),
        dma((n_z, n_tp)), dma((n_z,)), dma((-(-sends[0] // n_tp),)), dma((-(-sends[1] // n_tp),)),
        dma, dma((3,)),
        dma((n_z,)), dma((n_z, 2, near)), dma((n_z,)),
        dma((n_z,)), dma,
    ]
    return pl.pallas_call(
        functools.partial(kernel, n_sp, n_tp, cap),
        out_shape=pltpu.VMEM((feats, pos), BF16),
        in_specs=[anywhere] * 17,
        out_specs=vmem,
        scratch_shapes=scratch,
        compiler_params=pltpu.CompilerParams(
            collective_id=0, has_side_effects=True,
            vmem_limit_bytes=64 * 1024 * 1024 - 65536 - 2 * feats * pos,
        ),
    )(
        stream, values_in, in_gate, out_gate, documents.reshape(1, pos), conv_taps,
        head_gain.reshape(1, chans), mix_weight, norm_gain.reshape(1, feats), routes.T,
        route_weight.T, expert_gate, expert_up, expert_down, shared_gate, shared_up, shared_down,
    )


def solution(mesh):
    in_specs = (
        P("tp", "sp"),
        P("tp", "sp"),
        P("tp", "sp"),
        P("tp", "sp"),
        P("sp"),
        P(None, "tp"),
        P("tp"),
        P("tp", None),
        P("tp"),
        P("sp", None),
        P("sp", None),
        P("sp", None, "tp"),
        P("sp", None, "tp"),
        P("sp", None, "tp"),
        P(None, "tp"),
        P(None, "tp"),
        P("tp", None),
    )
    body = functools.partial(local, mesh.shape["sp"], mesh.shape["tp"])
    return jax.shard_map(
        body, mesh=mesh, in_specs=in_specs, out_specs=P("tp", "sp"), check_vma=False
    )
```

```python
import functools

import jax
import jax.numpy as jnp
from jax import lax
from jax.experimental import pallas as pl
from jax.experimental.pallas import tpu as pltpu
from jax.sharding import PartitionSpec as P

HEAD = 64
CORES = 2
SUB = 8
EDGE = 16
epsilon = 1e-06
MESH = pl.DeviceIdType.MESH
F32 = jnp.float32
BF16 = jnp.bfloat16


def flipped(index, mask):
    bit = 1
    out = index
    while bit <= mask:
        if mask & bit:
            out = out + bit - 2 * bit * lax.rem(lax.div(index, bit), 2)
        bit *= 2
    return out


def dot(left, right):
    return jnp.dot(left, right, preferred_element_type=F32)


def silu(value):
    return value / (1.0 + jnp.exp(-value))


def column_of(row, width):
    return jnp.broadcast_to(row, (width, row.shape[1])).T


def kernel(
    n_sp, n_tp, cap, n_mid,
    stream_h, values_h, in_h, out_h, documents_h, taps_h, head_h, mix_weight,
    norm_h, routes_h, route_weight_h, expert_gate, expert_up, expert_down,
    shared_gate, shared_up, shared_down,
    out,
    stream, values_in, in_gate, out_gate, documents, conv_taps, head_gain,
    norm_gain, routes, route_weight, mix_w, gate_w, up_w, sgate_w, sup_w, sdown_w, down_w,
    tail_s, prev_r, prev_docs, mix_s, mix_r, hidden_v, x_all, ss_s, ss_r, meta_r,
    sh_s, sh_r, mid_all, part_v, place_v, column_v, early_v, acc_v, pr_s, pr_r, zr_s, zr_r,
    pool, load_sem, halo_send, halo_recv, mix_recv, ss_recv,
    meta_recv, xm_recv, xo_recv, xb_send, sh_recv,
    mid_recv, fwd_recv, pr_recv, zr_recv,
):
    sp = lax.axis_index("sp")
    tp = lax.axis_index("tp")
    z = lax.div(sp, CORES)
    core = lax.rem(sp, CORES)
    n_z = n_sp // CORES
    feats, pos = stream.shape
    chans = values_in.shape[0]
    width = feats * n_tp
    hid = gate_w.shape[1]
    partner = {"sp": z * CORES + 1 - core}
    peers = [flipped(tp, d) for d in range(1, n_tp)]
    square = n_tp == 4 and n_z == 4
    near = peers[:2] if square else peers
    layers = [flipped(z, d) for d in range(n_z)]
    inner = lax.div(z + 1, 2) == 1
    if square:
        layers[2:] = [jnp.where(inner, layers[3], layers[2]), jnp.where(inner, layers[2], layers[3])]
    mix_send, ss_send, meta_send, sh_send = (pool.at[i] for i in range(4))
    branch = [""]
    counts = {}

    def only(where, stage, *args):
        @pl.when(inner if where == "inner" else jnp.logical_not(inner))
        def _():
            branch[0] = where
            stage(*args)
            branch[0] = ""

    def far_own():
        for d in (3, 2):
            send(x_all.at[sp, tp], x_all.at[sp, tp], "x", xm_recv.at[z, tp],
                 {"sp": layers[d] * CORES + core})

    def onward(d, slice_of):
        block = x_all.at[layers[d] * CORES + core, slice_of]
        send(block, block, "x", xm_recv.at[layers[d], slice_of],
             {"sp": layers[2 if d < 2 else 1] * CORES + core})

    def across(d, slice_of):
        block = x_all.at[layers[d] * CORES + core, slice_of]
        send(block, block, "x", xo_recv.at[layers[d]], partner)

    def send(src, dst, kind, rsem, device):
        if isinstance(kind, str):
            key = (branch[0], kind)
            at = counts.get(key, 0)
            counts[key] = at + 1
            if kind == "mid":
                sem = pool.at[4 + at // (2 * n_tp)]
            else:
                sem = xb_send.at[at // n_tp] if branch[0] else pool.at[4 + n_mid + at // n_tp]
        else:
            sem = kind
        pltpu.make_async_remote_copy(
            src_ref=src, dst_ref=dst, send_sem=sem, recv_sem=rsem,
            device_id=device, device_id_type=MESH,
        ).start()

    def sent(like, sem):
        pltpu.make_async_remote_copy(
            src_ref=like, dst_ref=like, send_sem=sem, recv_sem=sem,
            device_id=partner, device_id_type=MESH,
        ).wait_send()

    def all_sent(where):
        for kind, size in (("x", n_tp), ("mid", 2 * n_tp)):
            left, at = counts.get((where, kind), 0), 0
            while left > 0:
                now = min(left, size)
                if kind == "x":
                    sem = xb_send.at[at] if where else pool.at[4 + n_mid + at]
                    sent(x_all.at[0, pl.ds(0, now)], sem)
                else:
                    sent(mid_all.at[0, pl.ds(0, now // 2)], pool.at[4 + at])
                left, at = left - now, at + 1

    def arrived(dst, rsem):
        pltpu.make_async_remote_copy(
            src_ref=dst, dst_ref=dst, send_sem=rsem, recv_sem=rsem,
            device_id=partner, device_id_type=MESH,
        ).wait_recv()

    loads = [
        pltpu.make_async_copy(src, dst, load_sem.at[i])
        for i, (src, dst) in enumerate([
            (mix_weight, mix_w), (shared_gate, sgate_w), (shared_up, sup_w),
            (shared_down, sdown_w), (expert_gate.at[0], gate_w), (expert_up.at[0], up_w),
            (expert_down.at[0], down_w),
        ])
    ]
    smalls = [
        pltpu.make_async_copy(src, dst, pool.at[i])
        for i, (src, dst) in enumerate([
            (values_h, values_in), (in_h, in_gate), (documents_h, documents), (out_h, out_gate),
            (taps_h, conv_taps), (head_h, head_gain), (routes_h, routes),
            (route_weight_h, route_weight), (stream_h, stream), (norm_h, norm_gain),
        ])
    ]

    barrier = pltpu.get_barrier_semaphore()
    for d in range(1, n_sp):
        pl.semaphore_signal(
            barrier, inc=1, device_id={"sp": lax.rem(sp + d, n_sp)}, device_id_type=MESH
        )
    for peer in peers:
        pl.semaphore_signal(barrier, inc=1, device_id={"tp": peer}, device_id_type=MESH)
    for copy in smalls:
        copy.start()
    loads[0].start()
    for copy in smalls[:3]:
        copy.wait()
    product = values_in[...].astype(F32) * in_gate[...].astype(F32)
    tail_s[...] = product.T[pos - SUB:, :]
    for copy in smalls[3:]:
        copy.wait()

    tap_rows = jnp.concatenate([conv_taps[...], jnp.zeros((SUB - 3, chans), F32)], axis=0).T
    taps = [jnp.broadcast_to(tap_rows[:, j:j + 1], (chans, pos)) for j in range(3)]
    docs = documents[...]
    lane_c = lax.broadcasted_iota(jnp.int32, (chans, pos), 1)
    lane_1 = lax.broadcasted_iota(jnp.int32, (1, pos), 1)

    def heads_of(before, docs_before):
        convolved = taps[2] * product
        for shift in (1, 2):
            moved = pltpu.roll(product, shift, 1)
            if before is not None:
                moved = jnp.where(lane_c < shift, pltpu.roll(before, shift, 1), moved)
            ids = jnp.where(lane_1 < shift, pltpu.roll(docs_before, shift, 1), pltpu.roll(docs, shift, 1))
            convolved = convolved + jnp.where(ids == docs, taps[2 - shift] * moved, 0.0)
        mixed = out_gate[...].astype(F32) * convolved
        heads = mixed.reshape(chans // HEAD, HEAD, pos)
        heads = heads * lax.rsqrt(jnp.mean(heads * heads, axis=1, keepdims=True) + epsilon)
        return (heads.reshape(chans, pos).T * head_gain[...]).astype(BF16)

    def mix(rows, heads_t):
        for b, peer in enumerate(peers + [tp]):
            cols = pl.ds(pl.multiple_of(peer * feats, feats), feats)
            mix_s[b, rows[0]:rows[1]] = dot(heads_t[rows[0]:rows[1]], mix_w[:, cols]).astype(BF16)

    def mix_part(b, rows, slot, i, rsem):
        part = pl.ds(rows[0], rows[1] - rows[0])
        send(mix_s.at[b, part], mix_r.at[slot, part], mix_send, mix_recv.at[rsem], {"tp": peers[i]})

    parts = ((EDGE, pos // 2), (pos // 2, pos))

    def mix_on(i):
        rows = slice(*parts[i])
        with jax.named_scope(f"w_mixd{i}"):
            arrived(mix_r.at[2, pl.ds(parts[i][0], parts[i][1] - parts[i][0])], mix_recv.at[2 + i])
        mix_s[1 - i, rows] = (mix_s[1 - i, rows].astype(F32) + mix_r[2, rows].astype(F32)).astype(BF16)
        mix_part(1 - i, parts[i], 1, 1 - i, 1)

    def send_mix(rows):
        part = pl.ds(rows[0], rows[1] - rows[0])
        for b, peer in enumerate(peers):
            send(mix_s.at[b, part], mix_r.at[b, part], mix_send, mix_recv.at[b], {"tp": peer})

    heads_t = heads_of(None, jnp.full((1, pos), -1, jnp.int32))
    loads[0].wait()
    for load in loads[1:]:
        load.start()
    mix((EDGE, pos), heads_t)
    with jax.named_scope("barrier"):
        pl.semaphore_wait(barrier, n_tp - 1 + n_sp - 1)
    after = {"sp": lax.rem(sp + 1, n_sp)}
    halo = [
        pltpu.make_async_remote_copy(
            src_ref=src, dst_ref=dst, send_sem=halo_send.at[i], recv_sem=halo_recv.at[i],
            device_id=after, device_id_type=MESH,
        )
        for i, (src, dst) in enumerate([
            (tail_s, prev_r.at[pl.ds(pos - SUB, SUB)]), (documents, prev_docs),
        ])
    ]

    @pl.when(sp < n_sp - 1)
    def _():
        for copy in halo:
            copy.start()

    if square:
        for i in range(2):
            mix_part(2, parts[i], 2, i, 2 + i)
        for i in range(2):
            mix_part(i, parts[i], 0, i, 0)
    else:
        send_mix((EDGE, pos))

    @pl.when(sp == 0)
    def _():
        prev_r[...] = jnp.zeros((pos, chans), F32)
        prev_docs[...] = jnp.full((1, pos), -1, jnp.int32)

    @pl.when(sp > 0)
    def _():
        prev_r[: pos - SUB, :] = jnp.zeros((pos - SUB, chans), F32)
        with jax.named_scope("w_halo"):
            for copy in halo:
                copy.wait_recv()

    heads_t = heads_of(prev_r[...].T, prev_docs[...])
    mix((0, EDGE), heads_t)
    if square:
        for b in (2, 0, 1):
            mix_part(b, (0, EDGE), b, b, 4)
        mix_on(0)
        mix_on(1)
    else:
        send_mix((0, EDGE))

    named = routes[...]
    weights = route_weight[...]
    meta_rows = meta_r.shape[1]
    at_row = lax.broadcasted_iota(jnp.int32, (meta_rows, pos), 0)
    table = jnp.zeros((meta_rows, pos), F32)
    for k in range(routes.shape[0]):
        table = table + jnp.where(at_row == named[k:k + 1, :], weights[k:k + 1, :], 0.0)
    stream_t = stream[...].astype(F32).T

    hidden = stream_t + mix_s[n_tp - 1].astype(F32)
    if square:
        with jax.named_scope("w_mix"):
            arrived(mix_r.at[0, pl.ds(EDGE, pos - EDGE)], mix_recv.at[0])
            arrived(mix_r.at[1, pl.ds(EDGE, pos - EDGE)], mix_recv.at[1])
            arrived(mix_r.at[2, pl.ds(0, 3 * EDGE)], mix_recv.at[4])
        hidden = hidden + mix_r[0].astype(F32) + mix_r[1].astype(F32)
        edge = mix_r[2, :EDGE].astype(F32)
        hidden = hidden + jnp.concatenate([edge, jnp.zeros((pos - EDGE, feats), F32)], axis=0)
    for b in range(0 if square else n_tp - 1):
        with jax.named_scope(f"w_mix{b}"):
            arrived(mix_r.at[b], mix_recv.at[b])
        hidden = hidden + mix_r[b].astype(F32)
    hidden_v[...] = hidden
    x_all[sp, tp] = (hidden * norm_gain[...]).astype(BF16)
    squares = jnp.sum(hidden * hidden, axis=1, keepdims=True)
    row = jnp.broadcast_to(squares, (pos, pos)).T[:SUB]
    ss_s[...] = row
    for b, peer in enumerate(peers):
        send(ss_s, ss_r.at[b], ss_send, ss_recv, {"tp": peer})
    own = x_all.at[sp, tp]
    for b, peer in enumerate(peers):
        send(own, own, "x", xm_recv.at[z, tp], {"tp": peer})
    for d in ([1] if square else range(1, n_z)):
        send(own, own, "x", xm_recv.at[z, tp], {"sp": layers[d] * CORES + core})
    if square:
        only("inner", far_own)
    across(0, tp)

    with jax.named_scope("w_ss"):
        arrived(ss_r, ss_recv)
    for b in range(n_tp - 1):
        row = row + ss_r[b]
    scale = lax.rsqrt(row[:1] / width + epsilon)
    meta_r[sp] = jnp.where(at_row == meta_rows - 1, scale, table)
    for d in range(1, n_sp):
        send(meta_r.at[sp], meta_r.at[sp], meta_send, meta_recv.at[sp],
             {"sp": lax.rem(sp + d, n_sp)})

    def fetch(d, b):
        with jax.named_scope(f"w_x{d}_{b}"):
            arrived(x_all.at[layers[d] * CORES + core, peers[b]], xm_recv.at[layers[d], peers[b]])
        across(d, peers[b])

    def fetch_inner(d, b):
        fetch(d, b)
        onward(d, peers[b])

    def from_layer(d):
        block = x_all.at[layers[d] * CORES + core, tp]
        with jax.named_scope(f"w_layer{d}"):
            arrived(block, xm_recv.at[layers[d], tp])
        for b, peer in enumerate([] if square and d != 2 else near):
            send(block, block, "x", xm_recv.at[layers[d], tp], {"tp": peer})
        across(d, tp)

    def from_layer_inner(d):
        from_layer(d)
        if d != 2:
            onward(d, tp)

    def closer(b):
        block = x_all.at[sp, peers[b]]
        send(block, block, "x", xm_recv.at[z, peers[b]], {"sp": layers[1] * CORES + core})

    if square:
        only("inner", from_layer_inner, 1)

    with jax.named_scope("w_load"):
        for i in (1, 2, 3):
            loads[i].wait()
    scale_own = column_of(scale, pos)[:, :1]

    def shared_part(peer):
        rows = pl.ds(pl.multiple_of(peer * feats, feats), feats)
        block = x_all[sp, peer]
        return dot(block, sgate_w[rows, :]), dot(block, sup_w[rows, :])

    gate, upward = shared_part(tp)
    for b in range(n_tp - 1):
        fetch(0, b)
        if square:
            closer(b)
        if square and b == 2:
            only("inner", onward, 0, peers[2])
            only("end", from_layer, 2)
        more = shared_part(peers[b])
        gate, upward = gate + more[0], upward + more[1]
    shared_mid = (silu(gate * scale_own) * (upward * scale_own)).astype(BF16)
    half = pos // 2

    def shared_to(b, part, slot, i):
        part = pl.ds(part * half, half)
        rsem = sh_recv.at[1 + i] if slot == 2 else sh_recv.at[0]
        send(sh_s.at[b, part], sh_r.at[slot, part], sh_send, rsem, {"tp": peers[i]})

    for b in ([2, 0, 1, 3] if square else range(n_tp)):
        peer = (peers + [tp])[b]
        cols = pl.ds(pl.multiple_of(peer * feats, feats), feats)
        sh_s[b] = dot(shared_mid, sdown_w[:, cols]).astype(BF16)
        if square and b == 2:
            shared_to(2, 0, 2, 0)
            shared_to(2, 1, 2, 1)
        elif square and b < 2:
            shared_to(b, b, 0, b)
        elif b < n_tp - 1:
            send(sh_s.at[b], sh_r.at[b], sh_send, sh_recv.at[0], {"tp": peer})

    def shared_on(i):
        rows = slice(i * half, (i + 1) * half)
        with jax.named_scope(f"w_shared{i}"):
            arrived(sh_r.at[2, pl.ds(i * half, half)], sh_recv.at[1 + i])
        sh_s[1 - i, rows] = (sh_s[1 - i, rows].astype(F32) + sh_r[2, rows].astype(F32)).astype(BF16)
        shared_to(1 - i, i, 1, 1 - i)

    with jax.named_scope("w_load2"):
        for i in (4, 5, 6):
            loads[i].wait()

    at_a = lax.broadcasted_iota(jnp.int32, (pos, pos), 0)
    at_b = lax.broadcasted_iota(jnp.int32, (pos, pos), 1)
    earlier = jnp.where(at_a < at_b, 1.0, 0.0).astype(BF16)
    rank_row = lax.broadcasted_iota(jnp.int32, (cap, pos), 0).astype(F32)
    rank_lane = lax.broadcasted_iota(jnp.int32, (pos, cap), 1).astype(F32)

    def groups_of(d):
        return layers[d] * CORES + core, layers[d] * CORES + 1 - core

    def slots_of(group):
        weight = meta_r[group, pl.ds(sp, 1), :]
        mask = jnp.where(weight > 0.0, 1.0, 0.0)
        count = dot(jnp.broadcast_to(mask, (2 * SUB, pos)).astype(BF16), earlier)[:1]
        return weight, jnp.where(weight > 0.0, count, -1.0)

    def expert_part(group, peer):
        rows = pl.ds(pl.multiple_of(peer * feats, feats), feats)
        block = x_all[group, peer]
        return dot(block, gate_w[rows, :]), dot(block, up_w[rows, :])

    def begin(d):
        parts = [expert_part(groups_of(d)[0], peer) for peer in (tp, *near)]
        for i in range(2):
            early_v[i] = sum([part[i] for part in parts[1:]], parts[0][i])

    def widen(d, which=(0, 1), ready=False):
        groups = [groups_of(d)[i] for i in which]
        for i, group in zip(which, groups):
            with jax.named_scope(f"w_group{d}_{i}"):
                if d > 0 or i > 0:
                    arrived(meta_r.at[group], meta_recv.at[group])
                if i > 0:
                    arrived(x_all.at[group], xo_recv.at[layers[d]])
        rows = len(groups) * pos
        gate = jnp.zeros((rows, hid), F32)
        upward = jnp.zeros((rows, hid), F32)
        if ready:
            more = expert_part(groups[0], peers[2])
            gate, upward = early_v[0] + more[0], early_v[1] + more[1]
        for b in range(0 if ready else n_tp):
            block = jnp.concatenate([x_all[group, b] for group in groups], axis=0)
            gate = gate + dot(block, gate_w[b * feats:(b + 1) * feats, :])
            upward = upward + dot(block, up_w[b * feats:(b + 1) * feats, :])
        scales = jnp.concatenate([
            column_of(meta_r[group, meta_rows - 1:, :], pos)[:, :1] for group in groups
        ], axis=0)
        middle = (silu(gate * scales) * (upward * scales)).astype(BF16)
        for at, (i, group) in enumerate(zip(which, groups)):
            slot = slots_of(group)[1]
            pick = jnp.where(rank_row == slot, 1.0, 0.0).astype(BF16)
            mid_all[d, tp, i * cap:(i + 1) * cap, :] = dot(
                pick, middle[at * pos:(at + 1) * pos]
            ).astype(BF16)

    def mids(d, i):
        block = mid_all.at[d, tp, pl.ds(i * cap, cap)]
        for b, peer in enumerate(near):
            send(block, block, "mid", mid_recv.at[d, i, b], {"tp": peer})

    def relay(d, i):
        for b, peer in enumerate(near):
            part = mid_all.at[d, peer, pl.ds(i * cap, cap)]
            with jax.named_scope(f"w_mid{d}_{i}_{b}"):
                arrived(part, mid_recv.at[d, i, b])
            if square and b == i:
                send(part, part, "mid", fwd_recv.at[d], {"tp": near[1 - b]})

    def down(d, peer):
        rows = pl.ds(pl.multiple_of(peer * hid, hid), hid)
        return dot(mid_all[d, peer], down_w[rows, :])

    def gather(d):
        total = down(d, tp)
        for peer in near:
            total = total + down(d, peer)
        part_v[d] = total
        for i, group in enumerate(groups_of(d)):
            weight, slot = slots_of(group)
            place_v[d, i] = jnp.where(rank_lane == column_of(slot, cap), 1.0, 0.0).astype(BF16)
            column_v[d, i] = column_of(weight, pos)

    def narrow(d):
        if square:
            with jax.named_scope(f"w_fwd{d}"):
                arrived(mid_all.at[d, peers[2]], fwd_recv.at[d])
        total = part_v[d]
        if square:
            total = total + down(d, peers[2])
        total = total.astype(BF16)
        for i in (1, 0):
            term = dot(place_v[d, i], total[i * cap:(i + 1) * cap]) * column_v[d, i][:, :1]
            if i == 1:
                pr_s[d] = term.astype(BF16)
                send(pr_s.at[d], pr_r.at[d], "x", pr_recv.at[d], partner)
            else:
                acc_v[d] = term

    def join(d):
        with jax.named_scope(f"w_pr{d}"):
            arrived(pr_r.at[d], pr_recv.at[d])
        if d == 0:
            return
        total = acc_v[d] + pr_r[d].astype(F32)
        zr_s[d] = total.astype(BF16)
        slot = {"inner": (0, 1, 1), "end": (0, 2, 2)}[branch[0]][d - 1] if square else d - 1
        send(zr_s.at[d], zr_r.at[slot], "x", zr_recv, {"sp": layers[d] * CORES + core})

    def finish():
        result = hidden_v[...] + sh_s[n_tp - 1].astype(F32)
        blocks = 2 if square else n_tp - 1
        with jax.named_scope("w_sh"):
            arrived(sh_r.at[pl.ds(0, blocks)], sh_recv.at[0])
        for b in range(blocks):
            result = result + sh_r[b].astype(F32)
        result = result + acc_v[0] + pr_r[0].astype(F32)
        if n_z > 1:
            with jax.named_scope("w_zr"):
                arrived(zr_r, zr_recv)
        for d in range(1, n_z):
            result = result + zr_r[d - 1].astype(F32)
        out[...] = result.T.astype(BF16)
        with jax.named_scope("w_sent"):
            all_sent(branch[0])

    def run(plan):
        for stage, *where in plan:
            stage(*where)

    if square:
        plan = [(from_layer, 1), (widen, 0), (mids, 0, 0), (mids, 0, 1)]
        plan += [(fetch, 1, b) for b in range(3)] + [(shared_on, 0), (shared_on, 1)]
        plan += [(widen, 1), (mids, 1, 0), (mids, 1, 1), (relay, 0, 0), (relay, 0, 1), (from_layer, 3)]
        plan += [(fetch, 2, b) for b in range(3)] + [(widen, 2), (mids, 2, 0), (mids, 2, 1)]
        plan += [(relay, 1, 0), (relay, 1, 1), (fetch, 3, 0), (fetch, 3, 1), (begin, 3), (fetch, 3, 2)]
        plan += [(widen, 3, (0,), True), (mids, 3, 0), (widen, 3, (1,)), (mids, 3, 1)]
        plan += [(relay, 2, 0), (relay, 2, 1), (gather, 1), (narrow, 1), (gather, 2), (relay, 3, 0), (join, 1)]
        plan += [(gather, 0), (relay, 3, 1), (gather, 3), (narrow, 2), (join, 2), (narrow, 3)]
        plan += [(narrow, 0), (join, 3), (join, 0), (finish,)]
        only("end", run, plan)
        plan = [(from_layer_inner, 2), (from_layer_inner, 3), (widen, 0), (mids, 0, 0), (fetch_inner, 2, 2)]
        plan += [(fetch_inner, 1, b) for b in range(3)] + [(fetch, 2, 0), (fetch, 2, 1)]
        plan += [(shared_on, 0), (shared_on, 1), (widen, 1), (mids, 1, 0)]
        plan += [(widen, 2), (mids, 2, 0), (mids, 2, 1), (mids, 1, 1)]
        plan += [(fetch_inner, 3, b) for b in range(3)] + [(widen, 3), (mids, 3, 0), (mids, 3, 1)]
        plan += [(relay, 2, 0), (relay, 2, 1), (gather, 2), (relay, 3, 0), (relay, 3, 1)]
        plan += [(relay, 1, 0), (relay, 1, 1), (mids, 0, 1), (relay, 0, 0), (narrow, 2), (gather, 3)]
        plan += [(narrow, 3), (join, 2), (gather, 1), (join, 3), (narrow, 1), (join, 1)]
        plan += [(relay, 0, 1), (gather, 0), (narrow, 0), (join, 0), (finish,)]
        only("inner", run, plan)
    else:
        plan = [(from_layer, d) for d in range(1, n_z)]
        for d in range(n_z):
            plan += [(fetch, d, b) for b in range(n_tp - 1)] if d else []
            plan += [(widen, d), (mids, d, 0), (mids, d, 1)]
        for d in range(n_z):
            plan += [(relay, d, 0), (relay, d, 1), (gather, d), (narrow, d), (join, d)]
        run(plan + [(finish,)])

    with jax.named_scope("w_send"):
        all_sent("")
        sent(mix_s.at[pl.ds(0, n_tp - 1)], mix_send)
        sent(ss_r, ss_send)
        sent(meta_r.at[pl.ds(0, n_sp - 1)], meta_send)
        sent(sh_s.at[pl.ds(0, 3 if square else n_tp - 1)], sh_send)

        @pl.when(sp < n_sp - 1)
        def _():
            for copy in halo:
                copy.wait_send()


def local(n_sp, n_tp, *args):
    (stream, values_in, in_gate, out_gate, documents, conv_taps, head_gain, mix_weight,
     norm_gain, routes, route_weight, expert_gate, expert_up, expert_down,
     shared_gate, shared_up, shared_down) = args
    feats, pos = stream.shape
    chans = values_in.shape[0]
    width = feats * n_tp
    hid = expert_gate.shape[2]
    n_z = n_sp // CORES
    meta_rows = -(-(n_sp + 1) // SUB) * SUB
    experts = n_sp * expert_gate.shape[0]
    bound = 3 * pos * routes.shape[1] // (2 * experts)
    cap = -(-bound // (2 * SUB)) * 2 * SUB
    square = n_tp == 4 and n_z == 4
    near = 2 if square else n_tp - 1
    sends = (11, 34) if square else (n_tp * (2 * n_z + 1) * 2, 1)
    n_mid = 3 if square else n_z
    vmem = pl.BlockSpec(memory_space=pltpu.VMEM)
    anywhere = pl.BlockSpec(memory_space=pl.ANY)
    dma = pltpu.SemaphoreType.DMA
    scratch = [
        pltpu.VMEM((feats, pos), BF16),
        pltpu.VMEM((chans, pos), BF16),
        pltpu.VMEM((chans, pos), BF16),
        pltpu.VMEM((chans, pos), BF16),
        pltpu.VMEM((1, pos), jnp.int32),
        pltpu.VMEM(conv_taps.shape, F32),
        pltpu.VMEM((1, chans), F32),
        pltpu.VMEM((1, feats), F32),
        pltpu.VMEM((routes.shape[1], pos), jnp.int32),
        pltpu.VMEM((routes.shape[1], pos), F32),
        pltpu.VMEM((chans, width), BF16),
        pltpu.VMEM((width, hid), BF16),
        pltpu.VMEM((width, hid), BF16),
        pltpu.VMEM((width, hid), BF16),
        pltpu.VMEM((width, hid), BF16),
        pltpu.VMEM((hid, width), BF16),
        pltpu.VMEM((n_tp * hid, feats), BF16),
        pltpu.VMEM((SUB, chans), F32),
        pltpu.VMEM((pos, chans), F32),
        pltpu.VMEM((1, pos), jnp.int32),
        pltpu.VMEM((n_tp, pos, feats), BF16),
        pltpu.VMEM((n_tp, pos, feats), BF16),
        pltpu.VMEM((pos, feats), F32),
        pltpu.VMEM((n_sp, n_tp, pos, feats), BF16),
        pltpu.VMEM((SUB, pos), F32),
        pltpu.VMEM((n_tp - 1, SUB, pos), F32),
        pltpu.VMEM((n_sp, meta_rows, pos), F32),
        pltpu.VMEM((n_tp, pos, feats), BF16),
        pltpu.VMEM((n_tp, pos, feats), BF16),
        pltpu.VMEM((n_z, n_tp, CORES * cap, hid), BF16),
        pltpu.VMEM((n_z, CORES * cap, feats), F32),
        pltpu.VMEM((n_z, CORES, pos, cap), BF16),
        pltpu.VMEM((n_z, CORES, pos, pos), F32),
        pltpu.VMEM((2, pos, hid), F32),
        pltpu.VMEM((n_z, pos, feats), F32),
        pltpu.VMEM((n_z, pos, feats), BF16),
        pltpu.VMEM((n_z, pos, feats), BF16),
        pltpu.VMEM((n_z, pos, feats), BF16),
        pltpu.VMEM((max(n_z - 1, 1), pos, feats), BF16),
        dma((max(10, 4 + n_mid - (-sends[0] // n_tp)),)), dma((7,)),
        dma((2,)), dma((2,)),
        dma((max(n_tp - 1, 5),)), dma,
        dma((n_sp,)), dma((n_z, n_tp)), dma((n_z,)), dma((-(-sends[1] // n_tp),)), dma((3,)),
        dma((n_z, 2, near)), dma((n_z,)), dma((n_z,)), dma,
    ]
    return pl.pallas_call(
        functools.partial(kernel, n_sp, n_tp, cap, n_mid),
        out_shape=pltpu.VMEM((feats, pos), BF16),
        in_specs=[anywhere] * 17,
        out_specs=vmem,
        scratch_shapes=scratch,
        compiler_params=pltpu.CompilerParams(
            collective_id=0, has_side_effects=True,
            vmem_limit_bytes=64 * 1024 * 1024 - 65536 - 2 * feats * pos,
        ),
    )(
        stream, values_in, in_gate, out_gate, documents.reshape(1, pos), conv_taps,
        head_gain.reshape(1, chans), mix_weight, norm_gain.reshape(1, feats), routes.T,
        route_weight.T, expert_gate, expert_up, expert_down, shared_gate, shared_up, shared_down,
    )


def solution(mesh):
    in_specs = (
        P("tp", "sp"),
        P("tp", "sp"),
        P("tp", "sp"),
        P("tp", "sp"),
        P("sp"),
        P(None, "tp"),
        P("tp"),
        P("tp", None),
        P("tp"),
        P("sp", None),
        P("sp", None),
        P("sp", None, "tp"),
        P("sp", None, "tp"),
        P("sp", None, "tp"),
        P(None, "tp"),
        P(None, "tp"),
        P("tp", None),
    )
    body = functools.partial(local, mesh.shape["sp"], mesh.shape["tp"])
    return jax.shard_map(
        body, mesh=mesh, in_specs=in_specs, out_specs=P("tp", "sp"), check_vma=False
    )
```

```python
import functools

import jax
import jax.numpy as jnp
from jax import lax
from jax.experimental import pallas as pl
from jax.experimental.pallas import tpu as pltpu
from jax.sharding import PartitionSpec as P

HEAD = 64
CORES = 2
SUB = 8
EDGE = 16
epsilon = 1e-06
MESH = pl.DeviceIdType.MESH
F32 = jnp.float32
BF16 = jnp.bfloat16


def flipped(index, mask):
    bit = 1
    out = index
    while bit <= mask:
        if mask & bit:
            out = out + bit - 2 * bit * lax.rem(lax.div(index, bit), 2)
        bit *= 2
    return out


def dot(left, right):
    return jnp.dot(left, right, preferred_element_type=F32)


def silu(value):
    return value / (1.0 + jnp.exp(-value))


def column_of(row, width):
    return jnp.broadcast_to(row, (width, row.shape[1])).T


def kernel(
    n_sp, n_tp, cap, n_mid,
    stream_h, values_h, in_h, out_h, documents_h, taps_h, head_h, mix_weight,
    norm_h, routes_h, route_weight_h, expert_gate, expert_up, expert_down,
    shared_gate, shared_up, shared_down,
    out,
    stream, values_in, in_gate, out_gate, documents, conv_taps, head_gain,
    norm_gain, routes, route_weight, mix_w, gate_w, up_w, sgate_w, sup_w, sdown_w, down_w,
    tail_s, prev_r, prev_docs, mix_s, mix_r, hidden_v, x_all, ss_s, ss_r, meta_r,
    sh_s, sh_r, mid_all, part_v, place_v, column_v, early_v, acc_v, pr_s, pr_r, zr_s, zr_r,
    pool, load_sem, halo_send, halo_recv, mix_recv, ss_recv,
    meta_recv, xm_recv, xo_recv, sh_recv,
    mid_recv, fwd_recv, pr_recv, zr_recv,
):
    sp = lax.axis_index("sp")
    tp = lax.axis_index("tp")
    z = lax.div(sp, CORES)
    core = lax.rem(sp, CORES)
    n_z = n_sp // CORES
    feats, pos = stream.shape
    chans = values_in.shape[0]
    width = feats * n_tp
    hid = gate_w.shape[1]
    partner = {"sp": z * CORES + 1 - core}
    peers = [flipped(tp, d) for d in range(1, n_tp)]
    square = n_tp == 4 and n_z == 4
    near = peers[:2] if square else peers
    layers = [flipped(z, d) for d in range(n_z)]
    inner = lax.div(z + 1, 2) == 1
    if square:
        layers[2:] = [jnp.where(inner, layers[3], layers[2]), jnp.where(inner, layers[2], layers[3])]
    mix_send, ss_send, meta_send, sh_send = (pool.at[i] for i in range(4))
    branch = [""]
    counts = {}

    def only(where, stage, *args):
        @pl.when(inner if where == "inner" else jnp.logical_not(inner))
        def _():
            branch[0] = where
            stage(*args)
            branch[0] = ""

    def far_own():
        for d in (3, 2):
            send(x_all.at[sp, tp], x_all.at[sp, tp], "x", xm_recv.at[z, tp],
                 {"sp": layers[d] * CORES + core})

    def onward(d, slice_of):
        block = x_all.at[layers[d] * CORES + core, slice_of]
        send(block, block, "x", xm_recv.at[layers[d], slice_of],
             {"sp": layers[2 if d < 2 else 1] * CORES + core})

    def across(d, slice_of):
        block = x_all.at[layers[d] * CORES + core, slice_of]
        send(block, block, "x", xo_recv.at[layers[d]], partner)

    def send(src, dst, kind, rsem, device):
        if isinstance(kind, str):
            key = (branch[0], kind)
            at = counts.get(key, 0)
            counts[key] = at + 1
            if kind == "mid":
                sem = pool.at[4 + at // (2 * n_tp)]
            else:
                sem = load_sem.at[at // n_tp] if branch[0] else pool.at[4 + n_mid + at // n_tp]
        else:
            sem = kind
        pltpu.make_async_remote_copy(
            src_ref=src, dst_ref=dst, send_sem=sem, recv_sem=rsem,
            device_id=device, device_id_type=MESH,
        ).start()

    def sent(like, sem):
        pltpu.make_async_remote_copy(
            src_ref=like, dst_ref=like, send_sem=sem, recv_sem=sem,
            device_id=partner, device_id_type=MESH,
        ).wait_send()

    def all_sent(where):
        for kind, size in (("x", n_tp), ("mid", 2 * n_tp)):
            left, at = counts.get((where, kind), 0), 0
            while left > 0:
                now = min(left, size)
                if kind == "x":
                    sem = load_sem.at[at] if where else pool.at[4 + n_mid + at]
                    sent(x_all.at[0, pl.ds(0, now)], sem)
                else:
                    sent(mid_all.at[0, pl.ds(0, now // 2)], pool.at[4 + at])
                left, at = left - now, at + 1

    def arrived(dst, rsem):
        pltpu.make_async_remote_copy(
            src_ref=dst, dst_ref=dst, send_sem=rsem, recv_sem=rsem,
            device_id=partner, device_id_type=MESH,
        ).wait_recv()

    loads = [
        pltpu.make_async_copy(src, dst, load_sem.at[i])
        for i, (src, dst) in enumerate([
            (mix_weight, mix_w), (shared_gate, sgate_w), (shared_up, sup_w),
            (shared_down, sdown_w), (expert_gate.at[0], gate_w), (expert_up.at[0], up_w),
            (expert_down.at[0], down_w),
        ])
    ]
    smalls = [
        pltpu.make_async_copy(src, dst, pool.at[i])
        for i, (src, dst) in enumerate([
            (values_h, values_in), (in_h, in_gate), (documents_h, documents), (out_h, out_gate),
            (taps_h, conv_taps), (head_h, head_gain), (routes_h, routes),
            (route_weight_h, route_weight), (stream_h, stream), (norm_h, norm_gain),
        ])
    ]

    barrier = pltpu.get_barrier_semaphore()
    for d in range(1, n_sp):
        pl.semaphore_signal(
            barrier, inc=1, device_id={"sp": lax.rem(sp + d, n_sp)}, device_id_type=MESH
        )
    for peer in peers:
        pl.semaphore_signal(barrier, inc=1, device_id={"tp": peer}, device_id_type=MESH)
    for copy in smalls:
        copy.start()
    loads[0].start()
    for copy in smalls[:3]:
        copy.wait()
    product = values_in[...].astype(F32) * in_gate[...].astype(F32)
    tail_s[...] = product.T[pos - SUB:, :]
    for copy in smalls[3:]:
        copy.wait()

    tap_rows = jnp.concatenate([conv_taps[...], jnp.zeros((SUB - 3, chans), F32)], axis=0).T
    taps = [jnp.broadcast_to(tap_rows[:, j:j + 1], (chans, pos)) for j in range(3)]
    docs = documents[...]
    lane_c = lax.broadcasted_iota(jnp.int32, (chans, pos), 1)
    lane_1 = lax.broadcasted_iota(jnp.int32, (1, pos), 1)

    def heads_of(before, docs_before):
        convolved = taps[2] * product
        for shift in (1, 2):
            moved = pltpu.roll(product, shift, 1)
            if before is not None:
                moved = jnp.where(lane_c < shift, pltpu.roll(before, shift, 1), moved)
            ids = jnp.where(lane_1 < shift, pltpu.roll(docs_before, shift, 1), pltpu.roll(docs, shift, 1))
            convolved = convolved + jnp.where(ids == docs, taps[2 - shift] * moved, 0.0)
        mixed = out_gate[...].astype(F32) * convolved
        heads = mixed.reshape(chans // HEAD, HEAD, pos)
        heads = heads * lax.rsqrt(jnp.mean(heads * heads, axis=1, keepdims=True) + epsilon)
        return (heads.reshape(chans, pos).T * head_gain[...]).astype(BF16)

    def mix(rows, heads_t):
        for b, peer in enumerate(peers + [tp]):
            cols = pl.ds(pl.multiple_of(peer * feats, feats), feats)
            mix_s[b, rows[0]:rows[1]] = dot(heads_t[rows[0]:rows[1]], mix_w[:, cols]).astype(BF16)

    def mix_part(b, rows, slot, i, rsem):
        part = pl.ds(rows[0], rows[1] - rows[0])
        send(mix_s.at[b, part], mix_r.at[slot, part], mix_send, mix_recv.at[rsem], {"tp": peers[i]})

    parts = ((EDGE, pos // 2), (pos // 2, pos))

    def mix_on(i):
        rows = slice(*parts[i])
        with jax.named_scope(f"w_mixd{i}"):
            arrived(mix_r.at[2, pl.ds(parts[i][0], parts[i][1] - parts[i][0])], mix_recv.at[2 + i])
        mix_s[1 - i, rows] = (mix_s[1 - i, rows].astype(F32) + mix_r[2, rows].astype(F32)).astype(BF16)
        mix_part(1 - i, parts[i], 1, 1 - i, 1)

    def send_mix(rows):
        part = pl.ds(rows[0], rows[1] - rows[0])
        for b, peer in enumerate(peers):
            send(mix_s.at[b, part], mix_r.at[b, part], mix_send, mix_recv.at[b], {"tp": peer})

    heads_t = heads_of(None, jnp.full((1, pos), -1, jnp.int32))
    loads[0].wait()
    for load in loads[1:]:
        load.start()
    mix((EDGE, pos), heads_t)
    with jax.named_scope("barrier"):
        pl.semaphore_wait(barrier, n_tp - 1 + n_sp - 1)
    after = {"sp": lax.rem(sp + 1, n_sp)}
    halo = [
        pltpu.make_async_remote_copy(
            src_ref=src, dst_ref=dst, send_sem=halo_send.at[i], recv_sem=halo_recv.at[i],
            device_id=after, device_id_type=MESH,
        )
        for i, (src, dst) in enumerate([
            (tail_s, prev_r.at[pl.ds(pos - SUB, SUB)]), (documents, prev_docs),
        ])
    ]

    @pl.when(sp < n_sp - 1)
    def _():
        for copy in halo:
            copy.start()

    if square:
        for i in range(2):
            mix_part(2, parts[i], 2, i, 2 + i)
        for i in range(2):
            mix_part(i, parts[i], 0, i, 0)
    else:
        send_mix((EDGE, pos))

    @pl.when(sp == 0)
    def _():
        prev_r[...] = jnp.zeros((pos, chans), F32)
        prev_docs[...] = jnp.full((1, pos), -1, jnp.int32)

    @pl.when(sp > 0)
    def _():
        prev_r[: pos - SUB, :] = jnp.zeros((pos - SUB, chans), F32)
        with jax.named_scope("w_halo"):
            for copy in halo:
                copy.wait_recv()

    heads_t = heads_of(prev_r[...].T, prev_docs[...])
    mix((0, EDGE), heads_t)
    if square:
        for b in (2, 0, 1):
            mix_part(b, (0, EDGE), b, b, 4)
        mix_on(0)
        mix_on(1)
    else:
        send_mix((0, EDGE))

    named = routes[...]
    weights = route_weight[...]
    meta_rows = meta_r.shape[1]
    at_row = lax.broadcasted_iota(jnp.int32, (meta_rows, pos), 0)
    table = jnp.zeros((meta_rows, pos), F32)
    for k in range(routes.shape[0]):
        table = table + jnp.where(at_row == named[k:k + 1, :], weights[k:k + 1, :], 0.0)
    stream_t = stream[...].astype(F32).T

    for load in loads[1:]:
        load.wait()
    hidden = stream_t + mix_s[n_tp - 1].astype(F32)
    if square:
        with jax.named_scope("w_mix"):
            arrived(mix_r.at[0, pl.ds(EDGE, pos - EDGE)], mix_recv.at[0])
            arrived(mix_r.at[1, pl.ds(EDGE, pos - EDGE)], mix_recv.at[1])
            arrived(mix_r.at[2, pl.ds(0, 3 * EDGE)], mix_recv.at[4])
        hidden = hidden + mix_r[0].astype(F32) + mix_r[1].astype(F32)
        edge = mix_r[2, :EDGE].astype(F32)
        hidden = hidden + jnp.concatenate([edge, jnp.zeros((pos - EDGE, feats), F32)], axis=0)
    for b in range(0 if square else n_tp - 1):
        with jax.named_scope(f"w_mix{b}"):
            arrived(mix_r.at[b], mix_recv.at[b])
        hidden = hidden + mix_r[b].astype(F32)
    hidden_v[...] = hidden
    x_all[sp, tp] = (hidden * norm_gain[...]).astype(BF16)
    squares = jnp.sum(hidden * hidden, axis=1, keepdims=True)
    row = jnp.broadcast_to(squares, (pos, pos)).T[:SUB]
    ss_s[...] = row
    for b, peer in enumerate(peers):
        send(ss_s, ss_r.at[b], ss_send, ss_recv, {"tp": peer})
    own = x_all.at[sp, tp]
    for b, peer in enumerate(peers):
        send(own, own, "x", xm_recv.at[z, tp], {"tp": peer})
    for d in ([1] if square else range(1, n_z)):
        send(own, own, "x", xm_recv.at[z, tp], {"sp": layers[d] * CORES + core})
    if square:
        only("inner", far_own)
    across(0, tp)

    with jax.named_scope("w_ss"):
        arrived(ss_r, ss_recv)
    for b in range(n_tp - 1):
        row = row + ss_r[b]
    scale = lax.rsqrt(row[:1] / width + epsilon)
    meta_r[sp] = jnp.where(at_row == meta_rows - 1, scale, table)
    for d in range(1, n_sp):
        send(meta_r.at[sp], meta_r.at[sp], meta_send, meta_recv.at[sp],
             {"sp": lax.rem(sp + d, n_sp)})

    def fetch(d, b):
        with jax.named_scope(f"w_x{d}_{b}"):
            arrived(x_all.at[layers[d] * CORES + core, peers[b]], xm_recv.at[layers[d], peers[b]])
        across(d, peers[b])

    def fetch_inner(d, b):
        fetch(d, b)
        onward(d, peers[b])

    def from_layer(d):
        block = x_all.at[layers[d] * CORES + core, tp]
        with jax.named_scope(f"w_layer{d}"):
            arrived(block, xm_recv.at[layers[d], tp])
        for b, peer in enumerate([] if square and d != 2 else near):
            send(block, block, "x", xm_recv.at[layers[d], tp], {"tp": peer})
        across(d, tp)

    def from_layer_inner(d):
        from_layer(d)
        if d != 2:
            onward(d, tp)

    def closer(b):
        block = x_all.at[sp, peers[b]]
        send(block, block, "x", xm_recv.at[z, peers[b]], {"sp": layers[1] * CORES + core})

    if square:
        only("inner", from_layer_inner, 1)

    scale_own = column_of(scale, pos)[:, :1]

    def shared_part(peer):
        rows = pl.ds(pl.multiple_of(peer * feats, feats), feats)
        block = x_all[sp, peer]
        return dot(block, sgate_w[rows, :]), dot(block, sup_w[rows, :])

    gate, upward = shared_part(tp)
    for b in range(n_tp - 1):
        fetch(0, b)
        if square:
            closer(b)
        if square and b == 2:
            only("inner", onward, 0, peers[2])
            only("end", from_layer, 2)
        more = shared_part(peers[b])
        gate, upward = gate + more[0], upward + more[1]
    shared_mid = (silu(gate * scale_own) * (upward * scale_own)).astype(BF16)
    half = pos // 2

    def shared_to(b, part, slot, i):
        part = pl.ds(part * half, half)
        rsem = sh_recv.at[1 + i] if slot == 2 else sh_recv.at[0]
        send(sh_s.at[b, part], sh_r.at[slot, part], sh_send, rsem, {"tp": peers[i]})

    for b in ([2, 0, 1, 3] if square else range(n_tp)):
        peer = (peers + [tp])[b]
        cols = pl.ds(pl.multiple_of(peer * feats, feats), feats)
        sh_s[b] = dot(shared_mid, sdown_w[:, cols]).astype(BF16)
        if square and b == 2:
            shared_to(2, 0, 2, 0)
            shared_to(2, 1, 2, 1)
        elif square and b < 2:
            shared_to(b, b, 0, b)
        elif b < n_tp - 1:
            send(sh_s.at[b], sh_r.at[b], sh_send, sh_recv.at[0], {"tp": peer})

    def shared_on(i):
        rows = slice(i * half, (i + 1) * half)
        with jax.named_scope(f"w_shared{i}"):
            arrived(sh_r.at[2, pl.ds(i * half, half)], sh_recv.at[1 + i])
        sh_s[1 - i, rows] = (sh_s[1 - i, rows].astype(F32) + sh_r[2, rows].astype(F32)).astype(BF16)
        shared_to(1 - i, i, 1, 1 - i)


    at_a = lax.broadcasted_iota(jnp.int32, (pos, pos), 0)
    at_b = lax.broadcasted_iota(jnp.int32, (pos, pos), 1)
    earlier = jnp.where(at_a < at_b, 1.0, 0.0).astype(BF16)
    rank_row = lax.broadcasted_iota(jnp.int32, (cap, pos), 0).astype(F32)
    rank_lane = lax.broadcasted_iota(jnp.int32, (pos, cap), 1).astype(F32)

    def groups_of(d):
        return layers[d] * CORES + core, layers[d] * CORES + 1 - core

    def slots_of(group):
        weight = meta_r[group, pl.ds(sp, 1), :]
        mask = jnp.where(weight > 0.0, 1.0, 0.0)
        count = dot(jnp.broadcast_to(mask, (2 * SUB, pos)).astype(BF16), earlier)[:1]
        return weight, jnp.where(weight > 0.0, count, -1.0)

    def expert_part(group, peer):
        rows = pl.ds(pl.multiple_of(peer * feats, feats), feats)
        block = x_all[group, peer]
        return dot(block, gate_w[rows, :]), dot(block, up_w[rows, :])

    def begin(d):
        parts = [expert_part(groups_of(d)[0], peer) for peer in (tp, *near)]
        for i in range(2):
            early_v[i] = sum([part[i] for part in parts[1:]], parts[0][i])

    def widen(d, which=(0, 1), ready=False):
        groups = [groups_of(d)[i] for i in which]
        for i, group in zip(which, groups):
            with jax.named_scope(f"w_group{d}_{i}"):
                if d > 0 or i > 0:
                    arrived(meta_r.at[group], meta_recv.at[group])
                if i > 0:
                    arrived(x_all.at[group], xo_recv.at[layers[d]])
        rows = len(groups) * pos
        gate = jnp.zeros((rows, hid), F32)
        upward = jnp.zeros((rows, hid), F32)
        if ready:
            more = expert_part(groups[0], peers[2])
            gate, upward = early_v[0] + more[0], early_v[1] + more[1]
        for b in range(0 if ready else n_tp):
            block = jnp.concatenate([x_all[group, b] for group in groups], axis=0)
            gate = gate + dot(block, gate_w[b * feats:(b + 1) * feats, :])
            upward = upward + dot(block, up_w[b * feats:(b + 1) * feats, :])
        scales = jnp.concatenate([
            column_of(meta_r[group, meta_rows - 1:, :], pos)[:, :1] for group in groups
        ], axis=0)
        middle = (silu(gate * scales) * (upward * scales)).astype(BF16)
        for at, (i, group) in enumerate(zip(which, groups)):
            slot = slots_of(group)[1]
            pick = jnp.where(rank_row == slot, 1.0, 0.0).astype(BF16)
            mid_all[d, tp, i * cap:(i + 1) * cap, :] = dot(
                pick, middle[at * pos:(at + 1) * pos]
            ).astype(BF16)

    def mids(d, i):
        block = mid_all.at[d, tp, pl.ds(i * cap, cap)]
        for b, peer in enumerate(near):
            send(block, block, "mid", mid_recv.at[d, i, b], {"tp": peer})

    def relay(d, i):
        for b, peer in enumerate(near):
            part = mid_all.at[d, peer, pl.ds(i * cap, cap)]
            with jax.named_scope(f"w_mid{d}_{i}_{b}"):
                arrived(part, mid_recv.at[d, i, b])
            if square and b == i:
                send(part, part, "mid", fwd_recv.at[d], {"tp": near[1 - b]})

    def down(d, peer):
        rows = pl.ds(pl.multiple_of(peer * hid, hid), hid)
        return dot(mid_all[d, peer], down_w[rows, :])

    def gather(d):
        total = down(d, tp)
        for peer in near:
            total = total + down(d, peer)
        part_v[d] = total
        for i, group in enumerate(groups_of(d)):
            weight, slot = slots_of(group)
            place_v[d, i] = jnp.where(rank_lane == column_of(slot, cap), 1.0, 0.0).astype(BF16)
            column_v[d, i] = column_of(weight, pos)

    def narrow(d):
        if square:
            with jax.named_scope(f"w_fwd{d}"):
                arrived(mid_all.at[d, peers[2]], fwd_recv.at[d])
        total = part_v[d]
        if square:
            total = total + down(d, peers[2])
        total = total.astype(BF16)
        for i in (1, 0):
            term = dot(place_v[d, i], total[i * cap:(i + 1) * cap]) * column_v[d, i][:, :1]
            if i == 1:
                pr_s[d] = term.astype(BF16)
                send(pr_s.at[d], pr_r.at[d], "x", pr_recv.at[d], partner)
            else:
                acc_v[d] = term

    def join(d):
        with jax.named_scope(f"w_pr{d}"):
            arrived(pr_r.at[d], pr_recv.at[d])
        if d == 0:
            return
        total = acc_v[d] + pr_r[d].astype(F32)
        zr_s[d] = total.astype(BF16)
        slot = {"inner": (0, 1, 1), "end": (0, 2, 2)}[branch[0]][d - 1] if square else d - 1
        send(zr_s.at[d], zr_r.at[slot], "x", zr_recv, {"sp": layers[d] * CORES + core})

    def finish():
        result = hidden_v[...] + sh_s[n_tp - 1].astype(F32)
        blocks = 2 if square else n_tp - 1
        with jax.named_scope("w_sh"):
            arrived(sh_r.at[pl.ds(0, blocks)], sh_recv.at[0])
        for b in range(blocks):
            result = result + sh_r[b].astype(F32)
        result = result + acc_v[0] + pr_r[0].astype(F32)
        if n_z > 1:
            with jax.named_scope("w_zr"):
                arrived(zr_r, zr_recv)
        for d in range(1, n_z):
            result = result + zr_r[d - 1].astype(F32)
        out[...] = result.T.astype(BF16)
        with jax.named_scope("w_sent"):
            all_sent(branch[0])

    def run(plan):
        for stage, *where in plan:
            stage(*where)

    if square:
        plan = [(from_layer, 1), (widen, 0), (mids, 0, 0), (mids, 0, 1)]
        plan += [(fetch, 1, b) for b in range(3)] + [(shared_on, 0), (shared_on, 1)]
        plan += [(widen, 1), (mids, 1, 0), (mids, 1, 1), (from_layer, 3)]
        plan += [(fetch, 2, b) for b in range(3)] + [(widen, 2), (mids, 2, 0), (mids, 2, 1)]
        plan += [(relay, 1, 0), (relay, 1, 1), (fetch, 3, 0), (fetch, 3, 1), (begin, 3), (fetch, 3, 2)]
        plan += [(widen, 3, (0,), True), (mids, 3, 0), (widen, 3, (1,)), (mids, 3, 1)]
        plan += [(relay, 2, 0), (relay, 2, 1), (gather, 1), (narrow, 1), (gather, 2), (relay, 3, 0)]
        plan += [(join, 1), (relay, 3, 1), (relay, 0, 0), (relay, 0, 1), (gather, 3), (narrow, 2)]
        plan += [(join, 2), (narrow, 3), (gather, 0), (join, 3), (narrow, 0), (join, 0), (finish,)]
        only("end", run, plan)
        plan = [(from_layer_inner, 2), (from_layer_inner, 3), (widen, 0), (mids, 0, 0), (fetch_inner, 2, 2)]
        plan += [(fetch_inner, 1, b) for b in range(3)] + [(fetch, 2, 0), (fetch, 2, 1)]
        plan += [(shared_on, 0), (shared_on, 1), (widen, 1), (mids, 1, 0)]
        plan += [(widen, 2), (mids, 2, 0), (mids, 2, 1), (mids, 1, 1)]
        plan += [(fetch_inner, 3, b) for b in range(3)] + [(widen, 3), (mids, 3, 0), (mids, 3, 1)]
        plan += [(relay, 2, 0), (relay, 2, 1), (gather, 2), (relay, 3, 0), (relay, 3, 1)]
        plan += [(relay, 1, 0), (relay, 1, 1), (mids, 0, 1), (relay, 0, 0), (narrow, 2), (gather, 3)]
        plan += [(narrow, 3), (join, 2), (gather, 1), (join, 3), (narrow, 1), (join, 1)]
        plan += [(relay, 0, 1), (gather, 0), (narrow, 0), (join, 0), (finish,)]
        only("inner", run, plan)
    else:
        plan = [(from_layer, d) for d in range(1, n_z)]
        for d in range(n_z):
            plan += [(fetch, d, b) for b in range(n_tp - 1)] if d else []
            plan += [(widen, d), (mids, d, 0), (mids, d, 1)]
        for d in range(n_z):
            plan += [(relay, d, 0), (relay, d, 1), (gather, d), (narrow, d), (join, d)]
        run(plan + [(finish,)])

    with jax.named_scope("w_send"):
        all_sent("")
        sent(mix_s.at[pl.ds(0, n_tp - 1)], mix_send)
        sent(ss_r, ss_send)
        sent(meta_r.at[pl.ds(0, n_sp - 1)], meta_send)
        sent(sh_s.at[pl.ds(0, 3 if square else n_tp - 1)], sh_send)

        @pl.when(sp < n_sp - 1)
        def _():
            for copy in halo:
                copy.wait_send()


def local(n_sp, n_tp, *args):
    (stream, values_in, in_gate, out_gate, documents, conv_taps, head_gain, mix_weight,
     norm_gain, routes, route_weight, expert_gate, expert_up, expert_down,
     shared_gate, shared_up, shared_down) = args
    feats, pos = stream.shape
    chans = values_in.shape[0]
    width = feats * n_tp
    hid = expert_gate.shape[2]
    n_z = n_sp // CORES
    meta_rows = -(-(n_sp + 1) // SUB) * SUB
    experts = n_sp * expert_gate.shape[0]
    bound = 3 * pos * routes.shape[1] // (2 * experts)
    cap = -(-bound // (2 * SUB)) * 2 * SUB
    square = n_tp == 4 and n_z == 4
    near = 2 if square else n_tp - 1
    sends = (11, 34) if square else (n_tp * (2 * n_z + 1) * 2, 1)
    n_mid = 3 if square else n_z
    vmem = pl.BlockSpec(memory_space=pltpu.VMEM)
    anywhere = pl.BlockSpec(memory_space=pl.ANY)
    dma = pltpu.SemaphoreType.DMA
    scratch = [
        pltpu.VMEM((feats, pos), BF16),
        pltpu.VMEM((chans, pos), BF16),
        pltpu.VMEM((chans, pos), BF16),
        pltpu.VMEM((chans, pos), BF16),
        pltpu.VMEM((1, pos), jnp.int32),
        pltpu.VMEM(conv_taps.shape, F32),
        pltpu.VMEM((1, chans), F32),
        pltpu.VMEM((1, feats), F32),
        pltpu.VMEM((routes.shape[1], pos), jnp.int32),
        pltpu.VMEM((routes.shape[1], pos), F32),
        pltpu.VMEM((chans, width), BF16),
        pltpu.VMEM((width, hid), BF16),
        pltpu.VMEM((width, hid), BF16),
        pltpu.VMEM((width, hid), BF16),
        pltpu.VMEM((width, hid), BF16),
        pltpu.VMEM((hid, width), BF16),
        pltpu.VMEM((n_tp * hid, feats), BF16),
        pltpu.VMEM((SUB, chans), F32),
        pltpu.VMEM((pos, chans), F32),
        pltpu.VMEM((1, pos), jnp.int32),
        pltpu.VMEM((n_tp, pos, feats), BF16),
        pltpu.VMEM((n_tp, pos, feats), BF16),
        pltpu.VMEM((pos, feats), F32),
        pltpu.VMEM((n_sp, n_tp, pos, feats), BF16),
        pltpu.VMEM((SUB, pos), F32),
        pltpu.VMEM((n_tp - 1, SUB, pos), F32),
        pltpu.VMEM((n_sp, meta_rows, pos), F32),
        pltpu.VMEM((n_tp, pos, feats), BF16),
        pltpu.VMEM((n_tp, pos, feats), BF16),
        pltpu.VMEM((n_z, n_tp, CORES * cap, hid), BF16),
        pltpu.VMEM((n_z, CORES * cap, feats), F32),
        pltpu.VMEM((n_z, CORES, pos, cap), BF16),
        pltpu.VMEM((n_z, CORES, pos, pos), F32),
        pltpu.VMEM((2, pos, hid), F32),
        pltpu.VMEM((n_z, pos, feats), F32),
        pltpu.VMEM((n_z, pos, feats), BF16),
        pltpu.VMEM((n_z, pos, feats), BF16),
        pltpu.VMEM((n_z, pos, feats), BF16),
        pltpu.VMEM((max(n_z - 1, 1), pos, feats), BF16),
        dma((max(10, 4 + n_mid - (-sends[0] // n_tp)),)), dma((max(7, -(-sends[1] // n_tp)),)),
        dma((2,)), dma((2,)),
        dma((max(n_tp - 1, 5),)), dma,
        dma((n_sp,)), dma((n_z, n_tp)), dma((n_z,)), dma((3,)),
        dma((n_z, 2, near)), dma((n_z,)), dma((n_z,)), dma,
    ]
    return pl.pallas_call(
        functools.partial(kernel, n_sp, n_tp, cap, n_mid),
        out_shape=pltpu.VMEM((feats, pos), BF16),
        in_specs=[anywhere] * 17,
        out_specs=vmem,
        scratch_shapes=scratch,
        compiler_params=pltpu.CompilerParams(
            collective_id=0, has_side_effects=True,
            vmem_limit_bytes=64 * 1024 * 1024 - 65536 - 2 * feats * pos,
        ),
    )(
        stream, values_in, in_gate, out_gate, documents.reshape(1, pos), conv_taps,
        head_gain.reshape(1, chans), mix_weight, norm_gain.reshape(1, feats), routes.T,
        route_weight.T, expert_gate, expert_up, expert_down, shared_gate, shared_up, shared_down,
    )


def solution(mesh):
    in_specs = (
        P("tp", "sp"),
        P("tp", "sp"),
        P("tp", "sp"),
        P("tp", "sp"),
        P("sp"),
        P(None, "tp"),
        P("tp"),
        P("tp", None),
        P("tp"),
        P("sp", None),
        P("sp", None),
        P("sp", None, "tp"),
        P("sp", None, "tp"),
        P("sp", None, "tp"),
        P(None, "tp"),
        P(None, "tp"),
        P("tp", None),
    )
    body = functools.partial(local, mesh.shape["sp"], mesh.shape["tp"])
    return jax.shard_map(
        body, mesh=mesh, in_specs=in_specs, out_specs=P("tp", "sp"), check_vma=False
    )
```
